256 devices in a mesh: sp: 32 (over z, y), tp: 8 (over x, core).
Axes of the slice: x: 4, y: 4, z: 8, core: 2. Of those that a mesh axis runs over, the one named last changes fastest.
Arguments:
- resid_stream: bfloat16 [12288, 2048], P('sp'), may hold values from -6 to 6
- q_latent: bfloat16 [12288, 512], P('sp'), may hold values from -6 to 6
- kv_latent: bfloat16 [12288, 256], P('sp'), may hold values from -6 to 6
- rope_key: bfloat16 [12288, 64], P('sp'), may hold values from -6 to 6
- doc_ids: int32 [12288], P('sp'), may hold values from 0 to 3, as said below
- q_gain: float32 [512], replicated, may hold values from 1.5 to 64
- kv_gain: float32 [256], replicated, may hold values from 0.1 to 1.9
- w_query: bfloat16 [512, 3072], P(None, 'tp'), may hold values from -0.25 to 0.25
- w_key: bfloat16 [256, 2048], P(None, 'tp'), may hold values from -0.375 to 0.375
- w_value: bfloat16 [256, 2048], P(None, 'tp'), may hold values from -0.375 to 0.375
- w_out: bfloat16 [2048, 2048], replicated, may hold values from -0.5 to 0.5
- mix_gain: float32 [2048], replicated, may hold values from 0.1 to 1.9
- w_gate: bfloat16 [2048, 5632], P('sp', 'tp'), may hold values from -0.125 to 0.125
- w_up: bfloat16 [2048, 5632], P('sp', 'tp'), may hold values from -0.125 to 0.125
- w_down: bfloat16 [5632, 2048], P('tp', 'sp'), may hold values from -0.3125 to 0.3125
- out_gain: float32 [2048], replicated, may hold values from 0.1 to 1.9
Outputs:
- layer_out: bfloat16 [12288, 2048], P(('sp', 'tp'))
The draws below stay inside these ranges and needn't reach their ends.
Inputs may be any that keep to these rules, and one draw needn't show every extreme that they name: `doc_ids`: document numbers never fall along the sequence; every document has 1 to 9216 positions and one has exactly 9216.
All inputs are finite; a program needn't handle non-finite values.
Results may differ from the reference program's by a relative error of at most 0.02.
The reference program's roundings to bfloat16 on the way count: a program that leaves them out, or rounds other values in their place, can miss the bound.
Values may be sent and summed in bfloat16 or wider, within the bound.
A program may use at most 128 MiB of HBM per device.

```python
import math
import jax
import jax.numpy as jnp
from jax import lax

D = 2048
FF = 5632
HEADS = 16
NOPE = 128
RD = 64
VD = 128
QR = 512
KR = 256
TOK_DEV = 384
TOKENS = 12288
DOC_MOST = 9216
N_TP = 8


def draw_q_gain(key, part):
    return jnp.exp(jax.random.uniform(key, (QR,), jnp.float32, math.log(1.5), math.log(4.0)))


def draw_doc_ids(key, part):
    rest = TOKENS - DOC_MOST
    margin = max(1, rest // 6)
    key_slot = jax.random.fold_in(key, 11)
    key_first = jax.random.fold_in(key, 23)
    key_second = jax.random.fold_in(key, 37)
    big_slot = jax.random.randint(key_slot, (), 0, 4, dtype=jnp.int32)
    first_cut = jax.random.randint(key_first, (), margin, rest // 2, dtype=jnp.int32)
    second_cut = jax.random.randint(key_second, (), rest // 2 + margin, rest - margin + 1, dtype=jnp.int32)
    smaller = jnp.stack([first_cut, second_cut - first_cut, rest - second_cut]).astype(jnp.int32)
    slots = jnp.arange(4, dtype=jnp.int32)
    pick = slots - (slots > big_slot).astype(jnp.int32)
    pick = jnp.clip(pick, 0, 2)
    lengths = jnp.where(slots == big_slot, jnp.int32(DOC_MOST), jnp.take(smaller, pick))
    starts = jnp.cumsum(lengths).astype(jnp.int32)[:3]
    positions = jnp.arange(TOKENS, dtype=jnp.int32)
    return jnp.sum((positions[:, None] >= starts[None, :]).astype(jnp.int32), axis=1).astype(jnp.int32)


def shard_levels(stream_key, shape, split, low, largest):
    def one(axis_at, blocks):
        steps = jax.random.uniform(jax.random.fold_in(jax.random.fold_in(stream_key, 6), axis_at), (blocks,), jnp.float32, low / len(split), largest / len(split))
        return jnp.repeat(jnp.exp(steps), shape[axis_at] // blocks).reshape((-1,) + (1,) * (len(shape) - axis_at - 1))

    loudness = one(*split[0])
    for cut in split[1:]:
        loudness = loudness * one(*cut)
    return loudness


def normal_values(rng, dims, deviation, limit, shards=(), kind=jnp.bfloat16):
    values = jax.random.normal(rng, dims, jnp.float32) * deviation
    if len(shards) > 0:
        values = shard_levels(rng, dims, shards, -0.22, 0.18) * values
    return jnp.clip(values, min=-limit, max=limit).astype(kind)


def setup_inputs(seed: int = 0) -> dict:
    arg_keys = jax.random.split(jax.random.key(seed), 17)
    resid_stream = normal_values(arg_keys[0], (TOKENS, D), 1.0, 6.0, ((0, 32),))
    q_latent = normal_values(arg_keys[1], (TOKENS, QR), 1.0, 6.0, ((0, 32),))
    kv_latent = normal_values(arg_keys[2], (TOKENS, KR), 1.0, 6.0, ((0, 32),))
    rope_key = normal_values(arg_keys[3], (TOKENS, RD), 1.0, 6.0, ((0, 32),))
    doc_ids = draw_doc_ids(jax.random.fold_in(arg_keys[16], 71), 0)
    q_gain = draw_q_gain(jax.random.fold_in(arg_keys[16], 71), 0)
    kv_gain = jnp.clip(1.0 + 0.18 * jax.random.normal(arg_keys[6], (KR,), jnp.float32), 0.1, 1.9)
    w_query = normal_values(arg_keys[7], (QR, HEADS * (NOPE + RD)), QR ** -0.5, 0.25, ((1, 8),))
    w_key = normal_values(arg_keys[8], (KR, HEADS * NOPE), KR ** -0.5, 0.375, ((1, 8),))
    w_value = normal_values(arg_keys[9], (KR, HEADS * VD), KR ** -0.5, 0.375, ((1, 8),))
    w_out = normal_values(arg_keys[10], (HEADS * VD, D), (HEADS * VD // 16) ** -0.5, 0.5)
    mix_gain = jnp.clip(1.0 + 0.18 * jax.random.normal(arg_keys[11], (D,), jnp.float32), 0.1, 1.9)
    w_gate = normal_values(arg_keys[12], (D, FF), D ** -0.5, 0.125, ((0, 32), (1, 8)))
    w_up = normal_values(arg_keys[13], (D, FF), D ** -0.5, 0.125, ((0, 32), (1, 8)))
    w_down = normal_values(arg_keys[14], (FF, D), (FF // 16) ** -0.5, 0.3125, ((0, 8), (1, 32)))
    out_gain = jnp.clip(1.0 + 0.18 * jax.random.normal(arg_keys[15], (D,), jnp.float32), 0.1, 1.9)
    return dict(resid_stream=resid_stream, q_latent=q_latent, kv_latent=kv_latent, rope_key=rope_key, doc_ids=doc_ids, q_gain=q_gain, kv_gain=kv_gain, w_query=w_query, w_key=w_key, w_value=w_value, w_out=w_out, mix_gain=mix_gain, w_gate=w_gate, w_up=w_up, w_down=w_down, out_gain=out_gain)


eps_norm = 1e-05
rope_theta = 10000.0
resid_alpha = 8.0 ** 0.25

def rope_angles(positions):
    frequency = rope_theta ** (-jnp.arange(0, RD, 2, dtype=jnp.float32) / RD)
    angles = positions.astype(jnp.float32)[:, None] * frequency[None, :]
    return (jnp.cos(angles), jnp.sin(angles))

def rotate(values, cos_table, sin_table):
    half_width = values.shape[-1] // 2
    first_half = values[..., :half_width]
    second_half = values[..., half_width:]
    return jnp.concatenate([first_half * cos_table - second_half * sin_table, second_half * cos_table + first_half * sin_table], axis=-1)

def rms_scaled(latent, scaling):
    widened = latent.astype(jnp.float32)
    inverse = lax.rsqrt(lax.optimization_barrier(jnp.mean(widened * widened, axis=-1, keepdims=True)) + eps_norm)
    return (widened * inverse * scaling).astype(jnp.bfloat16)

def layer_scaled(stream, scaling):
    centre = stream - lax.optimization_barrier(jnp.mean(stream, axis=-1, keepdims=True))
    spread = lax.optimization_barrier(jnp.mean(centre * centre, axis=-1, keepdims=True))
    return centre * lax.rsqrt(spread + eps_norm) * scaling

def widen(packed):
    return lax.optimization_barrier(packed).astype(jnp.float32)

def reference(resid_stream, q_latent, kv_latent, rope_key, doc_ids, q_gain, kv_gain, w_query, w_key, w_value, w_out, mix_gain, w_gate, w_up, w_down, out_gain):
    positions = jnp.arange(TOKENS, dtype=jnp.int32)
    cos_table, sin_table = rope_angles(positions)
    q_normed = rms_scaled(q_latent, q_gain)
    queries = jnp.dot(q_normed, w_query, preferred_element_type=jnp.float32).reshape(TOKENS, HEADS, NOPE + RD)
    queries = jnp.concatenate([queries[:, :, :NOPE], rotate(queries[:, :, NOPE:], cos_table[:, None, :], sin_table[:, None, :])], axis=-1).astype(jnp.bfloat16)
    kv_normed = rms_scaled(kv_latent, kv_gain)
    key_nope = jnp.dot(kv_normed, w_key, preferred_element_type=jnp.float32).astype(jnp.bfloat16).reshape(TOKENS, HEADS, NOPE)
    values = jnp.dot(kv_normed, w_value, preferred_element_type=jnp.float32).astype(jnp.bfloat16).reshape(TOKENS, HEADS, VD)
    key_rot = rotate(rope_key.astype(jnp.float32), cos_table, sin_table).astype(jnp.bfloat16)
    score_scale = (NOPE + RD) ** (-0.5)
    key_wide = widen(key_nope)
    rot_wide = widen(key_rot)
    value_wide = widen(values)

    def one_block(block_index):
        first_row = (block_index * TOK_DEV).astype(jnp.int32)
        query_block = widen(lax.dynamic_slice_in_dim(queries, first_row, TOK_DEV, 0))
        doc_block = lax.dynamic_slice_in_dim(doc_ids, first_row, TOK_DEV, 0)
        scores = jnp.einsum('qhd,khd->hqk', query_block[:, :, :NOPE], key_wide)
        scores = (scores + jnp.einsum('qhd,kd->hqk', query_block[:, :, NOPE:], rot_wide)) * score_scale
        same_doc = (doc_block[:, None] == doc_ids[None, :])[None]
        masked = jnp.where(same_doc, scores, -1e+30)
        row_top = lax.optimization_barrier(jnp.max(masked, axis=-1, keepdims=True))
        weights = jnp.where(same_doc, jnp.exp(masked - row_top), 0.0)
        denom_sum = lax.optimization_barrier(jnp.sum(weights, axis=-1))
        weighted = jnp.einsum('hqk,khd->qhd', widen(weights.astype(jnp.bfloat16)), value_wide)
        return (weighted / jnp.transpose(denom_sum)[:, :, None]).astype(jnp.bfloat16)
    block_out = lax.map(one_block, jnp.arange(TOKENS // TOK_DEV, dtype=jnp.int32))
    attended = block_out.reshape(TOKENS, HEADS * VD)
    mixer_out = jnp.dot(attended, w_out, preferred_element_type=jnp.float32)
    normed_mid = layer_scaled(resid_alpha * resid_stream.astype(jnp.float32) + mixer_out, mix_gain).astype(jnp.bfloat16)
    gate_pre = jnp.dot(normed_mid, w_gate, preferred_element_type=jnp.float32)
    up_pre = jnp.dot(normed_mid, w_up, preferred_element_type=jnp.float32)
    hidden = (jax.nn.silu(gate_pre) * up_pre).astype(jnp.bfloat16)
    group_width = FF // N_TP
    ffn_sum = jnp.zeros((TOKENS, D), jnp.float32)
    for group_index in range(N_TP):
        partial_sum = jnp.dot(hidden[:, group_index * group_width:(group_index + 1) * group_width], w_down[group_index * group_width:(group_index + 1) * group_width, :], preferred_element_type=jnp.float32)
        ffn_sum = ffn_sum + widen(partial_sum.astype(jnp.bfloat16))
    layer_out = layer_scaled(resid_alpha * normed_mid.astype(jnp.float32) + 0.5 * ffn_sum, out_gain).astype(jnp.bfloat16)
    return layer_out
```

```python
import functools
import math

import jax
import jax.numpy as jnp
from jax import lax
from jax.experimental import pallas as pl
from jax.experimental.pallas import tpu as pltpu
from jax.sharding import Mesh
from jax.sharding import PartitionSpec as P

NOPE = 128
RD = 64
VD = 128
NZ, NY, NX, NC = 8, 4, 4, 2
SP = ("z", "y")
TP = ("x", "c")
MESH = pl.DeviceIdType.MESH

eps_norm = 1e-05
rope_theta = 10000.0
resid_alpha = 8.0**0.25
HEADS_DEV = 2
WIDE = 384
QUART = 96
EXP2_SCALE = (NOPE + RD) ** (-0.5) * math.log2(math.e)
F32 = jnp.float32
BF16 = jnp.bfloat16


def rope_angles(positions):
    frequency = rope_theta ** (-jnp.arange(0, RD, 2, dtype=jnp.float32) / RD)
    angles = positions.astype(jnp.float32)[:, None] * frequency[None, :]
    return (jnp.cos(angles), jnp.sin(angles))


def rotate(values, cos_table, sin_table):
    half_width = values.shape[-1] // 2
    first_half = values[..., :half_width]
    second_half = values[..., half_width:]
    return jnp.concatenate(
        [
            first_half * cos_table - second_half * sin_table,
            second_half * cos_table + first_half * sin_table,
        ],
        axis=-1,
    )


def rms_scaled(latent, scaling):
    widened = latent.astype(jnp.float32)
    inverse = lax.rsqrt(jnp.mean(widened * widened, axis=-1, keepdims=True) + eps_norm)
    return (widened * inverse * scaling).astype(jnp.bfloat16)


def layer_scaled(stream, scaling):
    centre = stream - jnp.mean(stream, axis=-1, keepdims=True)
    spread = jnp.mean(centre * centre, axis=-1, keepdims=True)
    return centre * lax.rsqrt(spread + eps_norm) * scaling


class Wires:
    def __init__(self):
        self.sent = []

    def copy(self, slot, pair, index, axis, target):
        send, recv = pair
        ref = slot()
        return pltpu.make_async_remote_copy(
            src_ref=ref,
            dst_ref=ref,
            send_sem=send.at[index],
            recv_sem=recv.at[index],
            device_id={axis: target},
            device_id_type=MESH,
        )

    def start(self, slot, pair, index, axis, target):
        self.copy(slot, pair, index, axis, target).start()
        self.sent.append((slot, pair, index, axis, target))

    def landed(self, slot, pair, index, axis, target):
        self.copy(slot, pair, index, axis, target).wait_recv()

    def finish(self):
        for item in self.sent:
            self.copy(*item).wait_send()


class RingYZ:
    SEMS = 12

    def __init__(self, wires, at, chunk, part, pair, me):
        self.w, self.at, self.chunk, self.part, self.pair = wires, at, chunk, part, pair
        z, y = me
        self.y = y
        self.yl, self.yr, self.yo = (y + 3) % 4, (y + 1) % 4, (y + 2) % 4
        self.zz = [lax.rem(z + d, 8) for d in range(8)]
        self.z = z

    def send(self, slot, index, axis, target):
        self.w.start(slot, self.pair, index, axis, target)

    def got(self, slot, index, axis="y"):
        target = self.yr if axis == "y" else self.zz[1]
        self.w.landed(slot, self.pair, index, axis, target)

    def y1(self):
        own = lambda: self.at(self.z, self.y)
        self.send(own, 0, "y", self.yr)
        self.send(own, 1, "y", self.yl)

    def y2(self):
        self.got(lambda: self.at(self.z, self.yl), 0)
        self.got(lambda: self.at(self.z, self.yr), 1)
        self.send(lambda: self.part(self.z, self.yl, 0), 2, "y", self.yr)
        self.send(lambda: self.part(self.z, self.yr, 1), 3, "y", self.yl)

    def z1(self):
        self.got(lambda: self.part(self.z, self.yo, 0), 2)
        self.got(lambda: self.part(self.z, self.yo, 1), 3)
        self.send(lambda: self.chunk(self.z, 0, 4), 4, "z", self.zz[1])
        self.send(lambda: self.chunk(self.z, 0, 4), 8, "z", self.zz[7])

    def zs(self, s):
        right, left = self.zz[9 - s], self.zz[s - 1]
        self.got(lambda: self.chunk(right, 0, 4), 4 + s - 2, "z")
        self.got(lambda: self.chunk(left, 0, 4), 8 + s - 2, "z")
        if s < 4:
            self.send(lambda: self.chunk(right, 0, 4), 4 + s - 1, "z", self.zz[1])
            self.send(lambda: self.chunk(left, 0, 4), 8 + s - 1, "z", self.zz[7])
        else:
            self.send(lambda: self.chunk(right, 0, 2), 7, "z", self.zz[1])
            self.send(lambda: self.chunk(left, 2, 4), 11, "z", self.zz[7])

    def z5(self):
        self.got(lambda: self.chunk(self.zz[4], 0, 2), 7, "z")
        self.got(lambda: self.chunk(self.zz[4], 2, 4), 11, "z")


class RingZY:
    SEMS = 40

    def __init__(self, wires, at, part, pair, me):
        self.w, self.at, self.part, self.pair = wires, at, part, pair
        z, y = me
        self.y = y
        self.yl, self.yr, self.yo = (y + 3) % 4, (y + 1) % 4, (y + 2) % 4
        self.zz = [lax.rem(z + d, 8) for d in range(8)]
        self.z = z

    def send(self, slot, index, axis, target):
        self.w.start(slot, self.pair, index, axis, target)

    def got(self, slot, index, axis):
        target = self.yr if axis == "y" else self.zz[1]
        self.w.landed(slot, self.pair, index, axis, target)

    def z1(self):
        own = lambda: self.at(self.z, self.y)
        self.send(own, 0, "z", self.zz[1])
        self.send(own, 4, "z", self.zz[7])

    def zs(self, s):
        right, left = self.zz[9 - s], self.zz[s - 1]
        self.got(lambda: self.at(right, self.y), s - 2, "z")
        self.got(lambda: self.at(left, self.y), 4 + s - 2, "z")
        if s < 4:
            self.send(lambda: self.at(right, self.y), s - 1, "z", self.zz[1])
            self.send(lambda: self.at(left, self.y), 4 + s - 1, "z", self.zz[7])
        else:
            self.send(lambda: self.part(right, self.y, 0), 3, "z", self.zz[1])
            self.send(lambda: self.part(left, self.y, 1), 7, "z", self.zz[7])

    def z5(self):
        self.got(lambda: self.part(self.zz[4], self.y, 0), 3, "z")
        self.got(lambda: self.part(self.zz[4], self.y, 1), 7, "z")

    def y1(self, d):
        zz = self.zz[d]
        self.send(lambda: self.at(zz, self.y), 8 + 4 * d, "y", self.yr)
        self.send(lambda: self.at(zz, self.y), 9 + 4 * d, "y", self.yl)

    def y2(self, d):
        zz = self.zz[d]
        self.got(lambda: self.at(zz, self.yl), 8 + 4 * d, "y")
        self.got(lambda: self.at(zz, self.yr), 9 + 4 * d, "y")
        self.send(lambda: self.part(zz, self.yl, 0), 10 + 4 * d, "y", self.yr)
        self.send(lambda: self.part(zz, self.yr, 1), 11 + 4 * d, "y", self.yl)

    def y3(self, d):
        zz = self.zz[d]
        self.got(lambda: self.part(zz, self.yo, 0), 10 + 4 * d, "y")
        self.got(lambda: self.part(zz, self.yo, 1), 11 + 4 * d, "y")


def layer_kernel(
    q_ref,
    kvm_ref,
    wg_ref,
    wu_ref,
    wd_ref,
    wkv_ref,
    att_ref,
    wa_out,
    wb_out,
    kv,
    wa,
    wb,
    m_ref,
    l_ref,
    acc_ref,
    loc_sem,
    ka_s,
    ka_r,
    kb_s,
    kb_r,
    kp_s,
    kp_r,
    wa_s,
    wa_r,
    wb_s,
    wb_r,
):
    z, y, c = lax.axis_index("z"), lax.axis_index("y"), lax.axis_index("c")
    other = 1 - c
    zz = [lax.rem(z + d, 8) for d in range(8)]

    own_rows = pl.multiple_of(c * 192, 96)
    local = [
        pltpu.make_async_copy(kvm_ref.at[pl.ds(own_rows, 96)], kv.at[0, c, z, y], loc_sem.at[0]),
        pltpu.make_async_copy(
            kvm_ref.at[pl.ds(own_rows + 96, 96)], kv.at[1, c, z, y], loc_sem.at[1]
        ),
        pltpu.make_async_copy(wg_ref, wa.at[z, y], loc_sem.at[2]),
        pltpu.make_async_copy(wu_ref, wb.at[z, y, 0], loc_sem.at[3]),
        pltpu.make_async_copy(wd_ref, wb.at[z, y, 1], loc_sem.at[4]),
    ]
    for copy in local:
        copy.start()

    barrier = pltpu.get_barrier_semaphore()
    for axis, target in (
        ("z", zz[1]),
        ("z", zz[7]),
        ("y", (y + 1) % 4),
        ("y", (y + 3) % 4),
        ("c", other),
    ):
        pl.semaphore_signal(barrier, inc=1, device_id={axis: target}, device_id_type=MESH)

    m_ref[...] = jnp.full(m_ref.shape, -1e30, F32)
    l_ref[...] = jnp.zeros(l_ref.shape, F32)
    acc_ref[...] = jnp.zeros(acc_ref.shape, F32)
    for copy in local:
        copy.wait()
    pl.semaphore_wait(barrier, 5)

    wires = Wires()
    half = lambda h: pl.ds(48 * h, 48)
    ka = RingYZ(
        wires,
        lambda a, b: kv.at[0, c, a, b],
        lambda a, lo, hi: kv.at[0, c, a, pl.ds(lo, hi - lo)],
        lambda a, b, h: kv.at[0, c, a, b, half(h)],
        (ka_s, ka_r),
        (z, y),
    )
    kb = RingZY(
        wires,
        lambda a, b: kv.at[1, c, a, b],
        lambda a, b, h: kv.at[1, c, a, b, half(h)],
        (kb_s, kb_r),
        (z, y),
    )
    ga = RingYZ(
        wires,
        lambda a, b: wa.at[a, b],
        lambda a, lo, hi: wa.at[a, pl.ds(lo, hi - lo)],
        lambda a, b, h: wa.at[a, b, pl.ds(32 * h, 32)],
        (wa_s, wa_r),
        (z, y),
    )
    gb = RingZY(
        wires,
        lambda a, b: wb.at[a, b],
        lambda a, b, h: wb.at[a, b, h],
        (wb_s, wb_r),
        (z, y),
    )

    def to_core(color, d):
        wires.start(lambda: kv.at[color, c, zz[d]], (kp_s, kp_r), 8 * color + d, "c", other)

    def attend(u):
        v = u + 2
        rnd, w = v // 4, v % 4
        color = w % 2
        d = lax.rem(jnp.where(w < 2, rnd, 8 - rnd), 8)
        at_z = lax.rem(z + d, 8)
        wires.landed(
            lambda: kv.at[color, other, at_z], (kp_s, kp_r), 8 * color + d, "c", other
        )
        x = kv[color, :, at_z].reshape(768, WIDE)
        extra = x[:, 256:384]
        both = jnp.dot(x[:, :256], wkv_ref[...], preferred_element_type=F32).astype(BF16)
        for h in range(HEADS_DEV):
            keys = jnp.concatenate([both[:, 128 * h : 128 * h + 128], extra], axis=1)
            vals = both[:, 256 + 128 * h : 384 + 128 * h]
            s = lax.dot_general(
                q_ref[h], keys, (((1,), (1,)), ((), ())), preferred_element_type=F32
            )
            top_old = m_ref[h]
            top = jnp.maximum(top_old, jnp.max(s, axis=1, keepdims=True))
            factor = jnp.exp2((top_old - top) * EXP2_SCALE)
            p = jnp.exp2((s - jnp.concatenate([top] * 6, axis=1)) * EXP2_SCALE)
            part = p[:, :128]
            for k in range(1, 6):
                part = part + p[:, 128 * k : 128 * k + 128]
            m_ref[h] = top
            l_ref[h] = l_ref[h] * factor + part
            acc_ref[h] = acc_ref[h] * factor + jnp.dot(
                p.astype(BF16), vals, preferred_element_type=F32
            )

    ka.y1()
    kb.z1()
    kb.y1(0)
    ka.y2()
    kb.zs(2)
    kb.y1(1)
    kb.y1(7)
    ka.z1()
    to_core(0, 0)
    kb.y2(0)
    kb.zs(3)
    kb.y1(2)
    kb.y1(6)
    kb.y3(0)
    to_core(1, 0)
    kb.y2(1)
    kb.y2(7)

    def event(u):
        if u == 2:
            kb.zs(4)
            kb.y1(3)
            kb.y1(5)
            ka.zs(2)
            to_core(0, 1)
            to_core(0, 7)
            kb.z5()
            kb.y1(4)
            kb.y3(1)
            kb.y3(7)
            to_core(1, 1)
            to_core(1, 7)
            kb.y2(2)
            kb.y2(6)
            ga.y1()
            gb.z1()
        if u == 6:
            ka.zs(3)
            to_core(0, 2)
            to_core(0, 6)
            kb.y3(2)
            kb.y3(6)
            to_core(1, 2)
            to_core(1, 6)
            kb.y2(3)
            kb.y2(5)
            ga.y2()
            gb.zs(2)
            gb.y1(0)
        if u == 10:
            ka.zs(4)
            to_core(0, 3)
            to_core(0, 5)
            kb.y3(3)
            kb.y3(5)
            to_core(1, 3)
            to_core(1, 5)
            kb.y2(4)
            ga.z1()
            gb.zs(3)
            gb.y1(1)
            gb.y1(7)
        if u == 14:
            ka.z5()
            to_core(0, 4)
            kb.y3(4)
            to_core(1, 4)
            gb.y2(0)
            gb.zs(4)
            gb.y1(2)
            gb.y1(6)

    def step(u, carry):
        for k in (2, 6, 10, 14):

            @pl.when(u == k)
            def _():
                event(k)

        attend(u)
        return carry

    lax.fori_loop(0, 16, step, 0)

    for h in range(HEADS_DEV):
        denom = jnp.sum(l_ref[h], axis=1, keepdims=True)
        att_ref[:, 128 * h : 128 * h + 128] = (acc_ref[h] / denom).astype(BF16)

    gb.z5()
    gb.y1(3)
    gb.y1(5)
    gb.y2(1)
    gb.y2(7)
    gb.y3(0)
    ga.zs(2)
    gb.y1(4)
    gb.y2(2)
    gb.y2(6)
    gb.y3(1)
    gb.y3(7)
    ga.zs(3)
    gb.y2(3)
    gb.y2(5)
    gb.y3(2)
    gb.y3(6)
    gb.y2(4)
    ga.zs(4)
    gb.y3(3)
    gb.y3(5)
    gb.y3(4)
    ga.z5()
    outs = [
        pltpu.make_async_copy(wa, wa_out, loc_sem.at[0]),
        pltpu.make_async_copy(wb, wb_out, loc_sem.at[1]),
    ]
    for copy in outs:
        copy.start()
    wires.finish()
    for copy in outs:
        copy.wait()


def body(
    resid_stream,
    q_latent,
    kv_latent,
    rope_key,
    doc_ids,
    q_gain,
    kv_gain,
    w_query,
    w_key,
    w_value,
    w_out,
    mix_gain,
    w_gate,
    w_up,
    w_down,
    out_gain,
):
    tok_rows = q_latent.shape[0]
    part_rows = tok_rows // (NX * NC)
    tp_index = lax.axis_index(TP)
    positions = lax.axis_index(SP) * tok_rows + jnp.arange(tok_rows, dtype=jnp.int32)
    cos_table, sin_table = rope_angles(positions)
    q_normed = rms_scaled(q_latent, q_gain)
    queries = jnp.dot(q_normed, w_query, preferred_element_type=jnp.float32).reshape(
        tok_rows, HEADS_DEV, NOPE + RD
    )
    kv_normed = rms_scaled(kv_latent, kv_gain)
    key_rot = rotate(rope_key.astype(jnp.float32), cos_table, sin_table).astype(jnp.bfloat16)
    slots = jnp.arange(64, dtype=jnp.int32)
    same = doc_ids[:, None] == slots[None, :]
    message = jnp.concatenate([kv_normed, key_rot, same.astype(BF16)], axis=1)
    apart = jnp.where(same | (slots >= 4)[None, :], 0.0, -1e30).astype(BF16)
    q_heads = []
    for h in range(HEADS_DEV):
        q_heads.append(
            jnp.concatenate(
                [
                    queries[:, h, :NOPE].astype(BF16),
                    rotate(queries[:, h, NOPE:], cos_table, sin_table).astype(BF16),
                    apart,
                ],
                axis=1,
            )
        )
    q_all = jnp.stack(q_heads)
    wkv = jnp.concatenate([w_key, w_value], axis=1)

    any_spec = pl.BlockSpec(memory_space=pl.ANY)
    vmem_spec = pl.BlockSpec(memory_space=pltpu.VMEM)
    dma = pltpu.SemaphoreType.DMA
    attended, wa, wb = pl.pallas_call(
        layer_kernel,
        out_shape=(
            jax.ShapeDtypeStruct((tok_rows, HEADS_DEV * VD), BF16),
            jax.ShapeDtypeStruct((NZ, NY, 64, 704), BF16),
            jax.ShapeDtypeStruct((NZ, NY, 2, 64, 704), BF16),
        ),
        in_specs=[vmem_spec, any_spec, any_spec, any_spec, any_spec, vmem_spec],
        out_specs=(vmem_spec, any_spec, any_spec),
        scratch_shapes=[
            pltpu.VMEM((2, NC, NZ, NY, QUART, WIDE), BF16),
            pltpu.VMEM((NZ, NY, 64, 704), BF16),
            pltpu.VMEM((NZ, NY, 2, 64, 704), BF16),
            pltpu.VMEM((HEADS_DEV, tok_rows, 128), F32),
            pltpu.VMEM((HEADS_DEV, tok_rows, 128), F32),
            pltpu.VMEM((HEADS_DEV, tok_rows, 128), F32),
            dma((8,)),
            dma((12,)),
            dma((12,)),
            dma((40,)),
            dma((40,)),
            dma((16,)),
            dma((16,)),
            dma((12,)),
            dma((12,)),
            dma((40,)),
            dma((40,)),
        ],
        compiler_params=pltpu.CompilerParams(
            collective_id=0, has_side_effects=True, vmem_limit_bytes=60 * 1024 * 1024
        ),
        name="gather_attend",
    )(q_all, message, w_gate, w_up, w_down.T, wkv)

    wg_all = wa.reshape(2048, 704)
    wu_all = wb[:, :, 0].reshape(2048, 704)
    wd_all = wb[:, :, 1].reshape(2048, 704)

    heads_rows = lax.all_to_all(attended, TP, split_axis=0, concat_axis=1, tiled=True)
    mixer_out = jnp.dot(heads_rows, w_out, preferred_element_type=jnp.float32)
    own_resid = lax.dynamic_slice_in_dim(resid_stream, tp_index * part_rows, part_rows, 0)
    own_normed = layer_scaled(
        resid_alpha * own_resid.astype(jnp.float32) + mixer_out, mix_gain
    ).astype(jnp.bfloat16)
    copies = jnp.broadcast_to(own_normed, (8, *own_normed.shape))
    normed_rows = lax.all_to_all(copies, TP, split_axis=0, concat_axis=0, tiled=True).reshape(
        tok_rows, 2048
    )
    gate_part = jnp.dot(normed_rows, wg_all, preferred_element_type=jnp.float32)
    up_part = jnp.dot(normed_rows, wu_all, preferred_element_type=jnp.float32)
    hidden = (jax.nn.silu(gate_part) * up_part).astype(jnp.bfloat16)
    down_term = lax.dot_general(
        hidden, wd_all, (((1,), (1,)), ((), ())), preferred_element_type=jnp.float32
    )
    tiles = lax.all_to_all(
        down_term.astype(BF16).reshape(8, part_rows, 2048), TP, 0, 0, tiled=True
    )
    ffn_sum = jnp.sum(tiles.astype(jnp.float32), axis=0)
    layer_out = layer_scaled(
        resid_alpha * own_normed.astype(jnp.float32) + 0.5 * ffn_sum, out_gain
    ).astype(jnp.bfloat16)
    return layer_out


def solution(mesh):
    split = Mesh(mesh.devices.reshape(NZ, NY, NX, NC), ("z", "y", "x", "c"))
    in_specs = (
        P(SP, None),
        P(SP, None),
        P(SP, None),
        P(SP, None),
        P(SP),
        P(),
        P(),
        P(None, TP),
        P(None, TP),
        P(None, TP),
        P(),
        P(),
        P(SP, TP),
        P(SP, TP),
        P(TP, SP),
        P(),
    )
    out_specs = P((*SP, *TP), None)
    return jax.shard_map(body, mesh=split, in_specs=in_specs, out_specs=out_specs, check_vma=False)
```

```python
import functools
import math

import jax
import jax.numpy as jnp
from jax import lax
from jax.experimental import pallas as pl
from jax.experimental.pallas import tpu as pltpu
from jax.sharding import Mesh
from jax.sharding import PartitionSpec as P

NOPE = 128
RD = 64
VD = 128
NZ, NY, NX, NC = 8, 4, 4, 2
SP = ("z", "y")
TP = ("x", "c")
MESH = pl.DeviceIdType.MESH

eps_norm = 1e-05
rope_theta = 10000.0
resid_alpha = 8.0**0.25
HEADS_DEV = 2
WIDE = 384
QUART = 96
EXP2_SCALE = (NOPE + RD) ** (-0.5) * math.log2(math.e)
F32 = jnp.float32
BF16 = jnp.bfloat16


def rope_angles(positions):
    frequency = rope_theta ** (-jnp.arange(0, RD, 2, dtype=jnp.float32) / RD)
    angles = positions.astype(jnp.float32)[:, None] * frequency[None, :]
    return (jnp.cos(angles), jnp.sin(angles))


def rotate(values, cos_table, sin_table):
    half_width = values.shape[-1] // 2
    first_half = values[..., :half_width]
    second_half = values[..., half_width:]
    return jnp.concatenate(
        [
            first_half * cos_table - second_half * sin_table,
            second_half * cos_table + first_half * sin_table,
        ],
        axis=-1,
    )


def rms_scaled(latent, scaling):
    widened = latent.astype(jnp.float32)
    inverse = lax.rsqrt(jnp.mean(widened * widened, axis=-1, keepdims=True) + eps_norm)
    return (widened * inverse * scaling).astype(jnp.bfloat16)


def layer_scaled(stream, scaling):
    centre = stream - jnp.mean(stream, axis=-1, keepdims=True)
    spread = jnp.mean(centre * centre, axis=-1, keepdims=True)
    return centre * lax.rsqrt(spread + eps_norm) * scaling


class Wires:
    def __init__(self, targets):
        self.targets = targets
        self.sent = []

    def copy(self, src, dst, pair, index, way):
        send, recv = pair
        return pltpu.make_async_remote_copy(
            src_ref=src(),
            dst_ref=dst(),
            send_sem=send.at[index],
            recv_sem=recv.at[index],
            device_id=self.targets[way],
            device_id_type=MESH,
        )

    def start(self, src, dst, pair, index, way, size):
        self.copy(src, dst, pair, index, way).start()
        self.sent.append((src, dst, pair, index, way))

    def landed(self, slot, pair, index, way):
        self.copy(slot, slot, pair, index, way).wait_recv()

    def finish(self):
        for item in self.sent:
            self.copy(*item).wait_send()


class Ring:
    def __init__(self, wires, pair, block, me, at, part, chunk=None):
        self.w, self.pair, self.block = wires, pair, block
        self.at, self.part, self.chunk = at, part, chunk
        self.z, self.y = me
        self.yl, self.yr, self.yo = (self.y + 3) % 4, (self.y + 1) % 4, (self.y + 2) % 4
        self.zz = [(self.z + d) % 8 for d in range(8)]

    def send(self, slot, index, way, blocks):
        self.w.start(slot, slot, self.pair, index, way, blocks * self.block)

    def got(self, slot, index, way="y+"):
        self.w.landed(slot, self.pair, index, way)


class RingYZ(Ring):
    def y1(self):
        own = lambda: self.at(self.z, self.y)
        self.send(own, 0, "y+", 1)
        self.send(own, 1, "y-", 1)

    def y2(self):
        self.got(lambda: self.at(self.z, self.yl), 0)
        self.got(lambda: self.at(self.z, self.yr), 1)
        self.send(lambda: self.part(self.z, self.yl, 0), 2, "y+", 0.5)
        self.send(lambda: self.part(self.z, self.yr, 1), 3, "y-", 0.5)

    def z1(self):
        self.got(lambda: self.part(self.z, self.yo, 0), 2)
        self.got(lambda: self.part(self.z, self.yo, 1), 3)
        self.send(lambda: self.chunk(self.z, 0, 4), 4, "z+", 4)
        self.send(lambda: self.chunk(self.z, 0, 4), 8, "z-", 4)

    def zs(self, s):
        right, left = self.zz[9 - s], self.zz[s - 1]
        self.got(lambda: self.chunk(right, 0, 4), 4 + s - 2)
        self.got(lambda: self.chunk(left, 0, 4), 8 + s - 2)
        if s < 4:
            self.send(lambda: self.chunk(right, 0, 4), 4 + s - 1, "z+", 4)
            self.send(lambda: self.chunk(left, 0, 4), 8 + s - 1, "z-", 4)
        else:
            self.send(lambda: self.chunk(right, 0, 2), 7, "z+", 2)
            self.send(lambda: self.chunk(left, 2, 4), 11, "z-", 2)

    def z5(self):
        self.got(lambda: self.chunk(self.zz[4], 0, 2), 7)
        self.got(lambda: self.chunk(self.zz[4], 2, 4), 11)


class RingZY(Ring):
    def z1(self):
        own = lambda: self.at(self.z, self.y)
        self.send(own, 0, "z+", 1)
        self.send(own, 4, "z-", 1)

    def zs(self, s):
        right, left = self.zz[9 - s], self.zz[s - 1]
        self.got(lambda: self.at(right, self.y), s - 2)
        self.got(lambda: self.at(left, self.y), 4 + s - 2)
        if s < 4:
            self.send(lambda: self.at(right, self.y), s - 1, "z+", 1)
            self.send(lambda: self.at(left, self.y), 4 + s - 1, "z-", 1)
        else:
            self.send(lambda: self.part(right, self.y, 0), 3, "z+", 0.5)
            self.send(lambda: self.part(left, self.y, 1), 7, "z-", 0.5)

    def z5(self):
        self.got(lambda: self.part(self.zz[4], self.y, 0), 3)
        self.got(lambda: self.part(self.zz[4], self.y, 1), 7)

    def y1(self, *steps):
        for d in steps:
            zz = self.zz[d]
            self.send(lambda zz=zz: self.at(zz, self.y), 8 + 4 * d, "y+", 1)
            self.send(lambda zz=zz: self.at(zz, self.y), 9 + 4 * d, "y-", 1)

    def y2(self, *steps):
        for d in steps:
            zz = self.zz[d]
            self.got(lambda zz=zz: self.at(zz, self.yl), 8 + 4 * d)
            self.got(lambda zz=zz: self.at(zz, self.yr), 9 + 4 * d)
            self.send(lambda zz=zz: self.part(zz, self.yl, 0), 10 + 4 * d, "y+", 0.5)
            self.send(lambda zz=zz: self.part(zz, self.yr, 1), 11 + 4 * d, "y-", 0.5)

    def y3(self, *steps):
        for d in steps:
            zz = self.zz[d]
            self.got(lambda zz=zz: self.part(zz, self.yo, 0), 10 + 4 * d)
            self.got(lambda zz=zz: self.part(zz, self.yo, 1), 11 + 4 * d)


def plan(ka, kb, ga, gb, share, attend, stage):
    ka.y1()
    kb.z1()
    kb.y1(0)
    ka.y2()
    kb.zs(2)
    kb.y1(1, 7)
    ka.z1()
    share(0, 0)
    kb.y2(0)
    kb.zs(3)
    kb.y1(2, 6)
    kb.y3(0)
    share(1, 0)
    kb.y2(1, 7)

    def at_2():
        kb.zs(4)
        kb.y1(3, 5)
        ka.zs(2)
        share(0, 1, 7)
        kb.z5()
        kb.y1(4)
        kb.y3(1, 7)
        share(1, 1, 7)
        kb.y2(2, 6)
        ga.y1()
        gb.z1()

    def at_6():
        ka.zs(3)
        share(0, 2, 6)
        kb.y3(2, 6)
        share(1, 2, 6)
        kb.y2(3, 5)
        ga.y2()
        gb.zs(2)
        gb.y1(0)

    def at_10():
        ka.zs(4)
        share(0, 3, 5)
        kb.y3(3, 5)
        share(1, 3, 5)
        kb.y2(4)
        ga.z1()
        gb.zs(3)
        gb.y1(1, 7)

    def at_14():
        ka.z5()
        share(0, 4)
        kb.y3(4)
        share(1, 4)
        gb.y2(0)
        gb.zs(4)
        gb.y1(2, 6)

    attend({2: at_2, 6: at_6, 10: at_10, 14: at_14})
    stage("heads")
    gb.z5()
    gb.y1(3, 5)
    gb.y2(1, 7)
    gb.y3(0)
    ga.zs(2)
    stage("mix")
    gb.y1(4)
    gb.y2(2, 6)
    gb.y3(1, 7)
    stage("norm")
    ga.zs(3)
    gb.y2(3, 5)
    gb.y3(2, 6)
    stage("spread")
    gb.y2(4)
    ga.zs(4)
    stage("spread2")
    gb.y3(3, 5, 4)
    ga.z5()
    stage("ffn")


def layer_kernel(
    q_ref,
    kvm_ref,
    wg_ref,
    wu_ref,
    wd_ref,
    wkv_ref,
    wo_ref,
    res_ref,
    gain_ref,
    out_ref,
    kv,
    wa,
    wb,
    m_ref,
    l_ref,
    acc_ref,
    att,
    heads,
    wo,
    res,
    mid,
    normed,
    gate,
    up,
    part,
    pin,
    xin,
    loc_sem,
    ka_s,
    ka_r,
    kb_s,
    kb_r,
    kp_s,
    kp_r,
    wa_s,
    wa_r,
    wb_s,
    wb_r,
    hd_s,
    hd_r,
    nx_s,
    nx_r,
    pp_s,
    pp_r,
    px_s,
    px_r,
):
    z, y = lax.axis_index("z"), lax.axis_index("y")
    x, c = lax.axis_index("x"), lax.axis_index("c")
    other = 1 - c
    zz = [(z + d) % 8 for d in range(8)]
    xr, xl, xo = (x + 1) % 4, (x + 3) % 4, (x + 2) % 4

    own_rows = pl.multiple_of(c * 192, 96)
    res_rows = pl.multiple_of((x * 2 + c) * 48, 48)
    local = [
        pltpu.make_async_copy(kvm_ref.at[pl.ds(own_rows, 96)], kv.at[0, c, z, y], loc_sem.at[0]),
        pltpu.make_async_copy(
            kvm_ref.at[pl.ds(own_rows + 96, 96)], kv.at[1, c, z, y], loc_sem.at[1]
        ),
        pltpu.make_async_copy(wg_ref, wa.at[z, y], loc_sem.at[2]),
        pltpu.make_async_copy(wu_ref, wb.at[z, y, 0], loc_sem.at[3]),
        pltpu.make_async_copy(wd_ref, wb.at[z, y, 1], loc_sem.at[4]),
    ]
    later = [
        pltpu.make_async_copy(wo_ref, wo, loc_sem.at[5]),
        pltpu.make_async_copy(res_ref.at[pl.ds(res_rows, 48)], res, loc_sem.at[6]),
    ]
    for copy in local + later:
        copy.start()

    targets = {
        "z+": {"z": zz[1]},
        "z-": {"z": zz[7]},
        "y+": {"y": (y + 1) % 4},
        "y-": {"y": (y + 3) % 4},
        "c": {"c": other},
    }
    for dx in range(4):
        for dc in range(2):
            if dx or dc:
                targets[dx, dc] = {"x": (x + dx) % 4, "c": (c + dc) % 2}
    targets["x+"], targets["x-"] = targets[1, 0], targets[3, 0]
    barrier = pltpu.get_barrier_semaphore()
    greeted = ["z+", "z-", "y+", "y-"] + [k for k in targets if isinstance(k, tuple)]
    for way in greeted:
        pl.semaphore_signal(barrier, inc=1, device_id=targets[way], device_id_type=MESH)

    m_ref[...] = jnp.full(m_ref.shape, -1e30, F32)
    l_ref[...] = jnp.zeros(l_ref.shape, F32)
    acc_ref[...] = jnp.zeros(acc_ref.shape, F32)
    for copy in local:
        copy.wait()
    pl.semaphore_wait(barrier, len(greeted))

    wires = Wires(targets)
    me = (z, y)
    kv_bytes, w_bytes = QUART * WIDE * 2, 64 * 768 * 2
    ka = RingYZ(
        wires,
        (ka_s, ka_r),
        kv_bytes,
        me,
        lambda a, b: kv.at[0, c, a, b],
        lambda a, b, h: kv.at[0, c, a, b, pl.ds(48 * h, 48)],
        lambda a, lo, hi: kv.at[0, c, a, pl.ds(lo, hi - lo)],
    )
    kb = RingZY(
        wires,
        (kb_s, kb_r),
        kv_bytes,
        me,
        lambda a, b: kv.at[1, c, a, b],
        lambda a, b, h: kv.at[1, c, a, b, pl.ds(48 * h, 48)],
    )
    ga = RingYZ(
        wires,
        (wa_s, wa_r),
        w_bytes,
        me,
        lambda a, b: wa.at[a, b],
        lambda a, b, h: wa.at[a, b, pl.ds(32 * h, 32)],
        lambda a, lo, hi: wa.at[a, pl.ds(lo, hi - lo)],
    )
    gb = RingZY(
        wires,
        (wb_s, wb_r),
        2 * w_bytes,
        me,
        lambda a, b: wb.at[a, b],
        lambda a, b, h: wb.at[a, b, h],
    )

    def share(color, *steps):
        for d in steps:
            slot = lambda d=d: kv.at[color, c, zz[d]]
            wires.start(slot, slot, (kp_s, kp_r), 8 * color + d, "c", 4 * kv_bytes)

    def attend_unit(u):
        v = u + 2
        rnd, w = v // 4, v % 4
        color = w % 2
        d = jnp.where(w < 2, rnd, 8 - rnd) % 8
        at_z = (z + d) % 8
        wires.landed(lambda: kv.at[color, other, at_z], (kp_s, kp_r), 8 * color + d, "c")
        rows = kv[color, :, at_z].reshape(768, WIDE)
        extra = rows[:, 256:384]
        both = jnp.dot(rows[:, :256], wkv_ref[...], preferred_element_type=F32).astype(BF16)
        for h in range(HEADS_DEV):
            keys = jnp.concatenate([both[:, 128 * h : 128 * h + 128], extra], axis=1)
            vals = both[:, 256 + 128 * h : 384 + 128 * h]
            s = lax.dot_general(
                q_ref[h], keys, (((1,), (1,)), ((), ())), preferred_element_type=F32
            )
            top_old = m_ref[h]
            top = jnp.maximum(top_old, jnp.max(s, axis=1, keepdims=True))
            factor = jnp.exp2((top_old - top) * EXP2_SCALE)
            p = jnp.exp2((s - jnp.concatenate([top] * 6, axis=1)) * EXP2_SCALE)
            total = p[:, :128]
            for k in range(1, 6):
                total = total + p[:, 128 * k : 128 * k + 128]
            m_ref[h] = top
            l_ref[h] = l_ref[h] * factor + total
            acc_ref[h] = acc_ref[h] * factor + jnp.dot(
                p.astype(BF16), vals, preferred_element_type=F32
            )

    def attend(events):
        def step(u, carry):
            for k, event in events.items():
                pl.when(u == k)(event)
            attend_unit(u)
            return carry

        lax.fori_loop(0, 16, step, 0)

    heads_pair, norm_pair = (hd_s, hd_r), (nx_s, nx_r)
    core_pair, x_pair = (pp_s, pp_r), (px_s, px_r)
    cols = lambda h: pl.ds(1024 * h, 1024)

    def pass_on(slot, index):
        wires.start(slot, slot, norm_pair, index, "c", 0)

    def stage(name):
        if name == "heads":
            for h in range(HEADS_DEV):
                denom = jnp.sum(l_ref[h], axis=1, keepdims=True)
                done = (acc_ref[h] / denom).astype(BF16)
                att[:, :, 128 * h : 128 * h + 128] = done.reshape(8, 48, 128)
            for dx in range(4):
                for dc in range(2):
                    if dx or dc:
                        there = (x + dx) % 4 * 2 + (c + dc) % 2
                        wires.start(
                            lambda there=there: att.at[there],
                            lambda: heads.at[x * 2 + c],
                            heads_pair,
                            2 * dx + dc,
                            (dx, dc),
                            0,
                        )
            heads[x * 2 + c] = att[x * 2 + c]
        if name == "mix":
            for dx in range(4):
                for dc in range(2):
                    if dx or dc:
                        there = (x - dx + 4) % 4 * 2 + (c + dc) % 2
                        wires.landed(
                            lambda: heads.at[there], heads_pair, 2 * dx + dc, (dx, dc)
                        )
            for copy in later:
                copy.wait()
            rows = jnp.concatenate([heads[j] for j in range(8)], axis=1)

            def mix(n, carry):
                at = pl.ds(pl.multiple_of(n * 256, 256), 256)
                mid[:, at] = jnp.dot(rows, wo[:, at], preferred_element_type=F32)
                return carry

            lax.fori_loop(0, 8, mix, 0)
        if name == "norm":
            stream = resid_alpha * res[...].astype(F32) + mid[...]
            normed[x, c] = layer_scaled(stream, gain_ref[0:1, :]).astype(BF16)
            own = lambda: normed.at[x, c]
            wires.start(own, own, norm_pair, 0, "x+", 0)
            wires.start(own, own, norm_pair, 1, "x-", 0)
            pass_on(own, 4)
        if name == "spread":
            wires.landed(lambda: normed.at[xl, c], norm_pair, 0, "x+")
            wires.landed(lambda: normed.at[xr, c], norm_pair, 1, "x-")
            slot = lambda: normed.at[xl, c, :, cols(0)]
            wires.start(slot, slot, norm_pair, 2, "x+", 0)
            slot_r = lambda: normed.at[xr, c, :, cols(1)]
            wires.start(slot_r, slot_r, norm_pair, 3, "x-", 0)
            pass_on(lambda: normed.at[xl, c], 5)
            pass_on(lambda: normed.at[xr, c], 6)
        if name == "spread2":
            wires.landed(lambda: normed.at[xo, c, :, cols(0)], norm_pair, 2, "x+")
            wires.landed(lambda: normed.at[xo, c, :, cols(1)], norm_pair, 3, "x-")
            pass_on(lambda: normed.at[xo, c], 7)
            for index, at in ((4, x), (5, xl), (6, xr), (7, xo)):
                wires.landed(lambda: normed.at[at, other], norm_pair, index, "c")
        if name == "ffn":
            for k in range(4):
                rows = normed[:, :, :, 512 * k : 512 * k + 512].reshape(384, 512)
                for w, total in (
                    (wa[2 * k : 2 * k + 2].reshape(512, 704), gate),
                    (wb[2 * k : 2 * k + 2, :, 0].reshape(512, 704), up),
                ):
                    term = jnp.dot(rows, w, preferred_element_type=F32)
                    total[...] = term if k == 0 else total[...] + term
            v = gate[...]
            hidden = (v / (1.0 + jnp.exp(-v)) * up[...]).astype(BF16)
            for k in range(8):
                w = wb[k, :, 1].reshape(256, 704)
                term = lax.dot_general(
                    hidden, w, (((1,), (1,)), ((), ())), preferred_element_type=F32
                )
                at = pl.ds(256 * k, 256)
                part[:, :, :, at] = term.astype(BF16).reshape(4, 2, 48, 256)
                wires.start(
                    lambda at=at: part.at[:, other, :, at],
                    lambda at=at: pin.at[:, :, at],
                    core_pair,
                    k,
                    "c",
                    0,
                )
            for k in range(8):
                wires.landed(lambda: pin.at[:, :, pl.ds(256 * k, 256)], core_pair, k, "c")

            def pair_sum(at_x, lo, hi):
                return part[at_x, c, :, lo:hi].astype(F32) + pin[at_x, :, lo:hi].astype(F32)

            def x_send(index, at_x, h, way):
                wires.start(
                    lambda: pin.at[at_x, :, cols(h)], lambda: xin.at[index], x_pair, index, way, 0
                )

            for at_x, h in ((xo, 0), (xo, 1), (xr, 1), (xl, 0)):
                half = slice(1024 * h, 1024 * h + 1024)
                pin[at_x, :, half] = pair_sum(at_x, half.start, half.stop).astype(BF16)
            x_send(0, xo, 0, "x+")
            x_send(1, xo, 1, "x-")
            x_send(2, xr, 1, "x+")
            x_send(3, xl, 0, "x-")
            near_r = pair_sum(xr, 0, 1024)
            near_l = pair_sum(xl, 1024, 2048)
            wires.landed(lambda: xin.at[0], x_pair, 0, "x+")
            pin[xr, :, 0:1024] = (near_r + xin[0].astype(F32)).astype(BF16)
            x_send(4, xr, 0, "x+")
            wires.landed(lambda: xin.at[1], x_pair, 1, "x-")
            pin[xl, :, 1024:2048] = (near_l + xin[1].astype(F32)).astype(BF16)
            x_send(5, xl, 1, "x-")
            for index, way in ((2, "x+"), (3, "x-"), (4, "x+"), (5, "x-")):
                wires.landed(lambda: xin.at[index], x_pair, index, way)
            low = pair_sum(x, 0, 1024) + xin[4].astype(F32) + xin[3].astype(F32)
            high = pair_sum(x, 1024, 2048) + xin[2].astype(F32) + xin[5].astype(F32)
            ffn_sum = jnp.concatenate([low, high], axis=1)
            stream = resid_alpha * normed[x, c].astype(F32) + 0.5 * ffn_sum
            out_ref[...] = layer_scaled(stream, gain_ref[1:2, :]).astype(BF16)

    plan(ka, kb, ga, gb, share, attend, stage)
    wires.finish()


def body(
    resid_stream,
    q_latent,
    kv_latent,
    rope_key,
    doc_ids,
    q_gain,
    kv_gain,
    w_query,
    w_key,
    w_value,
    w_out,
    mix_gain,
    w_gate,
    w_up,
    w_down,
    out_gain,
):
    tok_rows = q_latent.shape[0]
    positions = lax.axis_index(SP) * tok_rows + jnp.arange(tok_rows, dtype=jnp.int32)
    cos_table, sin_table = rope_angles(positions)
    q_normed = rms_scaled(q_latent, q_gain)
    queries = jnp.dot(q_normed, w_query, preferred_element_type=jnp.float32).reshape(
        tok_rows, HEADS_DEV, NOPE + RD
    )
    kv_normed = rms_scaled(kv_latent, kv_gain)
    key_rot = rotate(rope_key.astype(jnp.float32), cos_table, sin_table).astype(jnp.bfloat16)
    slots = jnp.arange(64, dtype=jnp.int32)
    same = doc_ids[:, None] == slots[None, :]
    message = jnp.concatenate([kv_normed, key_rot, same.astype(BF16)], axis=1)
    apart = jnp.where(same | (slots >= 4)[None, :], 0.0, -1e30).astype(BF16)
    q_heads = []
    for h in range(HEADS_DEV):
        q_heads.append(
            jnp.concatenate(
                [
                    queries[:, h, :NOPE].astype(BF16),
                    rotate(queries[:, h, NOPE:], cos_table, sin_table).astype(BF16),
                    apart,
                ],
                axis=1,
            )
        )
    q_all = jnp.stack(q_heads)
    wkv = jnp.concatenate([w_key, w_value], axis=1)

    any_spec = pl.BlockSpec(memory_space=pl.ANY)
    vmem_spec = pl.BlockSpec(memory_space=pltpu.VMEM)
    dma = pltpu.SemaphoreType.DMA
    vmem = pltpu.VMEM
    sizes = (12, 40, 16, 12, 40, 8, 8, 8, 6)
    return pl.pallas_call(
        layer_kernel,
        out_shape=jax.ShapeDtypeStruct((48, 2048), BF16),
        in_specs=[vmem_spec] + [any_spec] * 4 + [vmem_spec] + [any_spec] * 2 + [vmem_spec],
        out_specs=vmem_spec,
        scratch_shapes=[
            vmem((2, NC, NZ, NY, QUART, WIDE), BF16),
            vmem((NZ, NY, 64, 704), BF16),
            vmem((NZ, NY, 2, 64, 704), BF16),
            vmem((HEADS_DEV, tok_rows, 128), F32),
            vmem((HEADS_DEV, tok_rows, 128), F32),
            vmem((HEADS_DEV, tok_rows, 128), F32),
            vmem((8, 48, 256), BF16),
            vmem((8, 48, 256), BF16),
            vmem((2048, 2048), BF16),
            vmem((48, 2048), BF16),
            vmem((48, 2048), F32),
            vmem((NX, NC, 48, 2048), BF16),
            vmem((tok_rows, 704), F32),
            vmem((tok_rows, 704), F32),
            vmem((NX, NC, 48, 2048), BF16),
            vmem((NX, 48, 2048), BF16),
            vmem((6, 48, 1024), BF16),
            dma((8,)),
        ]
        + [dma((n,)) for n in sizes for _ in range(2)],
        compiler_params=pltpu.CompilerParams(
            collective_id=0, has_side_effects=True, vmem_limit_bytes=60 * 1024 * 1024
        ),
        name="whole_layer",
    )(
        q_all,
        message,
        w_gate,
        w_up,
        w_down.T,
        wkv,
        w_out,
        resid_stream,
        jnp.stack([mix_gain, out_gain]),
    )


def solution(mesh):
    split = Mesh(mesh.devices.reshape(NZ, NY, NX, NC), ("z", "y", "x", "c"))
    in_specs = (
        P(SP, None),
        P(SP, None),
        P(SP, None),
        P(SP, None),
        P(SP),
        P(),
        P(),
        P(None, TP),
        P(None, TP),
        P(None, TP),
        P(),
        P(),
        P(SP, TP),
        P(SP, TP),
        P(TP, SP),
        P(),
    )
    out_specs = P((*SP, *TP), None)
    return jax.shard_map(body, mesh=split, in_specs=in_specs, out_specs=out_specs, check_vma=False)
```

```python
import functools
import math

import jax
import jax.numpy as jnp
from jax import lax
from jax.experimental import pallas as pl
from jax.experimental.pallas import tpu as pltpu
from jax.sharding import Mesh
from jax.sharding import PartitionSpec as P

NOPE = 128
RD = 64
VD = 128
NZ, NY, NX, NC = 8, 4, 4, 2
SP = ("z", "y")
TP = ("x", "c")
MESH = pl.DeviceIdType.MESH

eps_norm = 1e-05
rope_theta = 10000.0
resid_alpha = 8.0**0.25
HEADS_DEV = 2
WIDE = 384
A_ROWS, B_ROWS = 64, 32
EXP2_SCALE = (NOPE + RD) ** (-0.5) * math.log2(math.e)
F32 = jnp.float32
BF16 = jnp.bfloat16


def rope_angles(positions):
    frequency = rope_theta ** (-jnp.arange(0, RD, 2, dtype=jnp.float32) / RD)
    angles = positions.astype(jnp.float32)[:, None] * frequency[None, :]
    return (jnp.cos(angles), jnp.sin(angles))


def rotate(values, cos_table, sin_table):
    half_width = values.shape[-1] // 2
    first_half = values[..., :half_width]
    second_half = values[..., half_width:]
    return jnp.concatenate(
        [
            first_half * cos_table - second_half * sin_table,
            second_half * cos_table + first_half * sin_table,
        ],
        axis=-1,
    )


def rms_scaled(latent, scaling):
    widened = latent.astype(jnp.float32)
    inverse = lax.rsqrt(jnp.mean(widened * widened, axis=-1, keepdims=True) + eps_norm)
    return (widened * inverse * scaling).astype(jnp.bfloat16)


def layer_scaled(stream, scaling):
    centre = stream - jnp.mean(stream, axis=-1, keepdims=True)
    spread = jnp.mean(centre * centre, axis=-1, keepdims=True)
    return centre * lax.rsqrt(spread + eps_norm) * scaling


class Wires:
    def __init__(self, targets):
        self.targets = targets
        self.sent = []

    def copy(self, src, dst, pair, index, way):
        send, recv = pair
        return pltpu.make_async_remote_copy(
            src_ref=src(),
            dst_ref=dst(),
            send_sem=send.at[index],
            recv_sem=recv.at[index],
            device_id=self.targets[way],
            device_id_type=MESH,
        )

    def start(self, src, dst, pair, index, way, size):
        self.copy(src, dst, pair, index, way).start()
        self.sent.append((src, dst, pair, index, way))

    def landed(self, slot, pair, index, way):
        self.copy(slot, slot, pair, index, way).wait_recv()

    def finish(self):
        for item in self.sent:
            self.copy(*item).wait_send()


class Ring:
    def __init__(self, wires, pair, block, me, at, part, chunk=None):
        self.w, self.pair, self.block = wires, pair, block
        self.at, self.part, self.chunk = at, part, chunk
        self.z, self.y = me
        self.yl, self.yr, self.yo = (self.y + 3) % 4, (self.y + 1) % 4, (self.y + 2) % 4
        self.zz = [(self.z + d) % 8 for d in range(8)]

    def send(self, slot, index, way, blocks):
        self.w.start(slot, slot, self.pair, index, way, blocks * self.block)

    def got(self, slot, index, way="y+"):
        self.w.landed(slot, self.pair, index, way)


class RingYZ(Ring):
    def y1(self):
        own = lambda: self.at(self.z, self.y)
        self.send(own, 0, "y+", 1)
        self.send(own, 1, "y-", 1)

    def y2(self):
        self.got(lambda: self.at(self.z, self.yl), 0)
        self.got(lambda: self.at(self.z, self.yr), 1)
        self.send(lambda: self.part(self.z, self.yl, 0), 2, "y+", 0.5)
        self.send(lambda: self.part(self.z, self.yr, 1), 3, "y-", 0.5)

    def z1(self):
        self.got(lambda: self.part(self.z, self.yo, 0), 2)
        self.got(lambda: self.part(self.z, self.yo, 1), 3)
        self.send(lambda: self.chunk(self.z, 0, 4), 4, "z+", 4)
        self.send(lambda: self.chunk(self.z, 0, 4), 8, "z-", 4)

    def zs(self, s):
        right, left = self.zz[9 - s], self.zz[s - 1]
        self.got(lambda: self.chunk(right, 0, 4), 4 + s - 2)
        self.got(lambda: self.chunk(left, 0, 4), 8 + s - 2)
        if s < 4:
            self.send(lambda: self.chunk(right, 0, 4), 4 + s - 1, "z+", 4)
            self.send(lambda: self.chunk(left, 0, 4), 8 + s - 1, "z-", 4)
        else:
            self.send(lambda: self.chunk(right, 0, 2), 7, "z+", 2)
            self.send(lambda: self.chunk(left, 2, 4), 11, "z-", 2)

    def z5(self):
        self.got(lambda: self.chunk(self.zz[4], 0, 2), 7)
        self.got(lambda: self.chunk(self.zz[4], 2, 4), 11)


class RingZY(Ring):
    def z1(self):
        own = lambda: self.at(self.z, self.y)
        self.send(own, 0, "z+", 1)
        self.send(own, 4, "z-", 1)

    def zs(self, s):
        right, left = self.zz[9 - s], self.zz[s - 1]
        self.got(lambda: self.at(right, self.y), s - 2)
        self.got(lambda: self.at(left, self.y), 4 + s - 2)
        if s < 4:
            self.send(lambda: self.at(right, self.y), s - 1, "z+", 1)
            self.send(lambda: self.at(left, self.y), 4 + s - 1, "z-", 1)
        else:
            self.send(lambda: self.part(right, self.y, 0), 3, "z+", 0.5)
            self.send(lambda: self.part(left, self.y, 1), 7, "z-", 0.5)

    def z5(self):
        self.got(lambda: self.part(self.zz[4], self.y, 0), 3)
        self.got(lambda: self.part(self.zz[4], self.y, 1), 7)

    def y1(self, *steps):
        for d in steps:
            zz = self.zz[d]
            self.send(lambda zz=zz: self.at(zz, self.y), 8 + 4 * d, "y+", 1)
            self.send(lambda zz=zz: self.at(zz, self.y), 9 + 4 * d, "y-", 1)

    def y2(self, *steps):
        for d in steps:
            zz = self.zz[d]
            self.got(lambda zz=zz: self.at(zz, self.yl), 8 + 4 * d)
            self.got(lambda zz=zz: self.at(zz, self.yr), 9 + 4 * d)
            self.send(lambda zz=zz: self.part(zz, self.yl, 0), 10 + 4 * d, "y+", 0.5)
            self.send(lambda zz=zz: self.part(zz, self.yr, 1), 11 + 4 * d, "y-", 0.5)

    def y3(self, *steps):
        for d in steps:
            zz = self.zz[d]
            self.got(lambda zz=zz: self.part(zz, self.yo, 0), 10 + 4 * d)
            self.got(lambda zz=zz: self.part(zz, self.yo, 1), 11 + 4 * d)


def plan(ka, kb, ga, gb, across, across2, attend, stage):
    ka.y1()
    kb.y1(0)
    kb.z1()
    gb.z1()
    gb.y1(0)
    kb.zs(2)
    kb.y1(1, 7)
    ka.y2()
    kb.y2(0)
    ga.y1()
    gb.zs(2)
    kb.zs(3)
    kb.y1(2, 6)
    kb.y2(1, 7)
    ka.z1()
    across(0, 0)
    kb.y3(0)
    across(1, 0)
    gb.y1(1)
    kb.y2(2, 6)
    kb.y3(1)
    across(1, 1)
    kb.y3(7)
    across(1, 7)
    across2(0, 0)
    kb.zs(4)
    kb.y1(3, 5)
    across2(1, 0)
    gb.zs(3)

    def at_0_1():
        across2(1, 1, 7)
        gb.y1(2)

    def at_1_0():
        ka.zs(2)
        across(0, 1, 7)
        kb.y3(6)
        across(1, 6)
        kb.y2(3)
        kb.z5()
        kb.y1(4)
        kb.y2(5)
        kb.y3(2)
        across(1, 2)
        gb.y2(1)
        across2(0, 1)
        gb.zs(4)
        gb.y1(5)
        kb.y3(3)
        across(1, 3)
        kb.y2(4)

    def at_1_1():
        across2(0, 7)
        kb.y3(5)
        across(1, 5)

    def at_2_0():
        across2(1, 6, 2)
        ka.zs(3)
        across(0, 2, 6)
        gb.y3(1)

    def at_2_1():
        across2(1, 3)
        gb.z5()
        gb.y1(4)

    def at_3_0():
        across2(1, 5)
        kb.y3(4)
        across(1, 4)
        across2(0, 2)
        ga.y2()

    def at_3_1():
        ka.zs(4)
        across(0, 3, 5)
        across2(0, 6)
        gb.y2(5)

    def at_4_0():
        across2(1, 4)
        gb.y1(3)
        ga.z1()

    def at_5_0():
        ka.z5()
        across(0, 4)
        across2(0, 3)
        gb.y3(5)
        gb.y2(2)
        across2(0, 5)

    def at_5_1():
        gb.y2(4)

    def at_6_0():
        across2(0, 4)
        gb.y1(7)

    def at_6_1():
        gb.y3(2)

    def at_7_0():
        ga.zs(2)
        gb.y3(4)

    def at_7_1():
        gb.y1(6)

    attend(
        {
            (0, 1): at_0_1,
            (1, 0): at_1_0,
            (1, 1): at_1_1,
            (2, 0): at_2_0,
            (2, 1): at_2_1,
            (3, 0): at_3_0,
            (3, 1): at_3_1,
            (4, 0): at_4_0,
            (5, 0): at_5_0,
            (5, 1): at_5_1,
            (6, 0): at_6_0,
            (6, 1): at_6_1,
            (7, 0): at_7_0,
            (7, 1): at_7_1,
        }
    )
    stage("heads")
    gb.y2(7, 0)
    stage("mix")
    gb.y2(6)
    ga.zs(3)
    gb.y3(7)
    stage("norm")
    gb.y2(3)
    gb.y3(0, 6, 3)
    stage("spread")
    ga.zs(4)
    stage("spread2")
    stage("gate0")
    stage("gate1")
    stage("gate2")
    ga.z5()
    stage("gate3")
    stage("ffn")


def layer_kernel(
    q_ref,
    kvm_ref,
    wg_ref,
    wu_ref,
    wd_ref,
    wkv_ref,
    wo_ref,
    res_ref,
    gain_ref,
    out_ref,
    kva,
    kvb,
    wa,
    wb,
    m_ref,
    l_ref,
    acc_ref,
    att,
    heads,
    wo,
    res,
    mid,
    normed,
    gate,
    up,
    part,
    pin,
    xin,
    loc_sem,
    ka_s,
    ka_r,
    kb_s,
    kb_r,
    kp_s,
    kp_r,
    kx_s,
    kx_r,
    wa_s,
    wa_r,
    wb_s,
    wb_r,
    hd_s,
    hd_r,
    nx_s,
    nx_r,
    pp_s,
    pp_r,
    px_s,
    px_r,
):
    z, y = lax.axis_index("z"), lax.axis_index("y")
    x, c = lax.axis_index("x"), lax.axis_index("c")
    other = 1 - c
    zz = [(z + d) % 8 for d in range(8)]
    xr, xl, xo = (x + 1) % 4, (x + 3) % 4, (x + 2) % 4

    par = x % 2
    apar = 1 - par
    own_rows = pl.multiple_of(c * 192 + par * 96, 32)
    res_rows = pl.multiple_of((x * 2 + c) * 48, 48)
    local = [
        pltpu.make_async_copy(
            kvm_ref.at[pl.ds(own_rows, A_ROWS)], kva.at[par, c, z, y], loc_sem.at[0]
        ),
        pltpu.make_async_copy(
            kvm_ref.at[pl.ds(own_rows + A_ROWS, B_ROWS)], kvb.at[par, c, z, y], loc_sem.at[1]
        ),
        pltpu.make_async_copy(wg_ref, wa.at[z, y], loc_sem.at[2]),
        pltpu.make_async_copy(wu_ref, wb.at[z, y, 0], loc_sem.at[3]),
        pltpu.make_async_copy(wd_ref, wb.at[z, y, 1], loc_sem.at[4]),
    ]
    later = [
        pltpu.make_async_copy(wo_ref, wo, loc_sem.at[5]),
        pltpu.make_async_copy(res_ref.at[pl.ds(res_rows, 48)], res, loc_sem.at[6]),
    ]
    for copy in local + later:
        copy.start()

    targets = {
        "z+": {"z": zz[1]},
        "z-": {"z": zz[7]},
        "y+": {"y": (y + 1) % 4},
        "y-": {"y": (y + 3) % 4},
        "c": {"c": other},
    }
    for dx in range(4):
        for dc in range(2):
            if dx or dc:
                targets[dx, dc] = {"x": (x + dx) % 4, "c": (c + dc) % 2}
    targets["x+"], targets["x-"] = targets[1, 0], targets[3, 0]
    barrier = pltpu.get_barrier_semaphore()
    greeted = ["z+", "z-", "y+", "y-"] + [k for k in targets if isinstance(k, tuple)]
    for way in greeted:
        pl.semaphore_signal(barrier, inc=1, device_id=targets[way], device_id_type=MESH)

    m_ref[...] = jnp.full(m_ref.shape, -1e30, F32)
    l_ref[...] = jnp.zeros(l_ref.shape, F32)
    acc_ref[...] = jnp.zeros(acc_ref.shape, F32)
    for copy in local:
        copy.wait()
    pl.semaphore_wait(barrier, len(greeted))

    wires = Wires(targets)
    me = (z, y)
    row_bytes, w_bytes = WIDE * 2, 64 * 768 * 2
    ka = RingYZ(
        wires,
        (ka_s, ka_r),
        A_ROWS * row_bytes,
        me,
        lambda a, b: kva.at[par, c, a, b],
        lambda a, b, h: kva.at[par, c, a, b, pl.ds(32 * h, 32)],
        lambda a, lo, hi: kva.at[par, c, a, pl.ds(lo, hi - lo)],
    )
    kb = RingZY(
        wires,
        (kb_s, kb_r),
        B_ROWS * row_bytes,
        me,
        lambda a, b: kvb.at[par, c, a, b],
        lambda a, b, h: kvb.at[par, c, a, b, pl.ds(16 * h, 16)],
    )
    ga = RingYZ(
        wires,
        (wa_s, wa_r),
        w_bytes,
        me,
        lambda a, b: wa.at[a, b],
        lambda a, b, h: wa.at[a, b, pl.ds(32 * h, 32)],
        lambda a, lo, hi: wa.at[a, pl.ds(lo, hi - lo)],
    )
    gb = RingZY(
        wires,
        (wb_s, wb_r),
        2 * w_bytes,
        me,
        lambda a, b: wb.at[a, b],
        lambda a, b, h: wb.at[a, b, h],
    )

    keys_of = (kva, kvb)

    def pair_with(color, d, theirs):
        own = apar if theirs else par
        slot = lambda: keys_of[color].at[own, c, zz[d]]
        wires.start(slot, slot, (kp_s, kp_r), 16 * theirs + 8 * color + d, "c", 0)

    def across(color, *steps):
        for d in steps:
            for h, way in ((0, "x+"), (1, "x-")):
                slot = lambda d=d, h=h: keys_of[color].at[par, c, zz[d], pl.ds(2 * h, 2)]
                wires.start(slot, slot, (kx_s, kx_r), 16 * h + 8 * color + d, way, 0)
            pair_with(color, d, 0)

    def across2(color, *steps):
        for d in steps:
            for h, way in ((0, "x+"), (1, "x-")):
                slot = lambda: keys_of[color].at[apar, c, zz[d], pl.ds(2 * h, 2)]
                wires.landed(slot, (kx_s, kx_r), 16 * h + 8 * color + d, way)
            pair_with(color, d, 1)

    def attend_unit(u, h):
        d = jnp.where(u % 2 == 1, (u + 1) // 2, (8 - u // 2) % 8)
        at_z = (z + d) % 8
        if h == 0:
            for theirs, own in ((0, par), (1, apar)):
                for color, keys in enumerate(keys_of):
                    wires.landed(
                        lambda: keys.at[own, other, at_z],
                        (kp_s, kp_r),
                        16 * theirs + 8 * color + d,
                        "c",
                    )
        rows = jnp.concatenate(
            [kva[:, :, at_z].reshape(1024, WIDE), kvb[:, :, at_z].reshape(512, WIDE)], axis=0
        )
        extra = rows[:, 256:384]
        both = jnp.dot(rows[:, :256], wkv_ref[h], preferred_element_type=F32).astype(BF16)
        keys = jnp.concatenate([both[:, :128], extra], axis=1)
        vals = both[:, 128:]
        s = lax.dot_general(
            q_ref[h], keys, (((1,), (1,)), ((), ())), preferred_element_type=F32
        )
        top_old = m_ref[h]
        top = jnp.maximum(top_old, jnp.max(s, axis=1, keepdims=True))
        factor = jnp.exp2((top_old - top) * EXP2_SCALE)
        p = jnp.exp2((s - jnp.concatenate([top] * 12, axis=1)) * EXP2_SCALE)
        total = p[:, :128]
        for k in range(1, 12):
            total = total + p[:, 128 * k : 128 * k + 128]
        m_ref[h] = top
        l_ref[h] = l_ref[h] * factor + total
        acc_ref[h] = acc_ref[h] * factor + jnp.dot(
            p.astype(BF16), vals, preferred_element_type=F32
        )

    def attend(events):
        def step(u, carry):
            for h in range(HEADS_DEV):
                for (k, at_h), event in events.items():
                    if at_h == h:
                        pl.when(u == k)(event)
                attend_unit(u, h)
            return carry

        lax.fori_loop(0, 8, step, 0)

    heads_pair, norm_pair = (hd_s, hd_r), (nx_s, nx_r)
    core_pair, x_pair = (pp_s, pp_r), (px_s, px_r)
    cols = lambda h: pl.ds(1024 * h, 1024)

    def pass_on(slot, index):
        wires.start(slot, slot, norm_pair, index, "c", 0)

    def stage(name):
        if name == "heads":
            for h in range(HEADS_DEV):
                denom = jnp.sum(l_ref[h], axis=1, keepdims=True)
                done = (acc_ref[h] / denom).astype(BF16)
                att[:, :, 128 * h : 128 * h + 128] = done.reshape(8, 48, 128)
            for dx in range(4):
                for dc in range(2):
                    if dx or dc:
                        there = (x + dx) % 4 * 2 + (c + dc) % 2
                        wires.start(
                            lambda there=there: att.at[there],
                            lambda: heads.at[x * 2 + c],
                            heads_pair,
                            2 * dx + dc,
                            (dx, dc),
                            0,
                        )
            heads[x * 2 + c] = att[x * 2 + c]
        if name == "mix":
            for dx in range(4):
                for dc in range(2):
                    if dx or dc:
                        there = (x - dx + 4) % 4 * 2 + (c + dc) % 2
                        wires.landed(
                            lambda: heads.at[there], heads_pair, 2 * dx + dc, (dx, dc)
                        )
            for copy in later:
                copy.wait()
            rows = jnp.concatenate([heads[j] for j in range(8)], axis=1)

            def mix(n, carry):
                at = pl.ds(pl.multiple_of(n * 256, 256), 256)
                mid[:, at] = jnp.dot(rows, wo[:, at], preferred_element_type=F32)
                return carry

            lax.fori_loop(0, 8, mix, 0)
        if name == "norm":
            stream = resid_alpha * res[...].astype(F32) + mid[...]
            normed[x, c] = layer_scaled(stream, gain_ref[0:1, :]).astype(BF16)
            own = lambda: normed.at[x, c]
            wires.start(own, own, norm_pair, 0, "x+", 0)
            wires.start(own, own, norm_pair, 1, "x-", 0)
            pass_on(own, 4)
        if name == "spread":
            wires.landed(lambda: normed.at[xl, c], norm_pair, 0, "x+")
            wires.landed(lambda: normed.at[xr, c], norm_pair, 1, "x-")
            slot = lambda: normed.at[xl, c, :, cols(0)]
            wires.start(slot, slot, norm_pair, 2, "x+", 0)
            slot_r = lambda: normed.at[xr, c, :, cols(1)]
            wires.start(slot_r, slot_r, norm_pair, 3, "x-", 0)
            pass_on(lambda: normed.at[xl, c], 5)
            pass_on(lambda: normed.at[xr, c], 6)
        if name == "spread2":
            wires.landed(lambda: normed.at[xo, c, :, cols(0)], norm_pair, 2, "x+")
            wires.landed(lambda: normed.at[xo, c, :, cols(1)], norm_pair, 3, "x-")
            pass_on(lambda: normed.at[xo, c], 7)
            for index, at in ((4, x), (5, xl), (6, xr), (7, xo)):
                wires.landed(lambda: normed.at[at, other], norm_pair, index, "c")
        if name[:4] == "gate":
            k = int(name[4:])
            near, far = ((0, 1), (7, 2), (6, 3), (5, 4))[k]
            at = [zz[near], zz[far]]
            rows = jnp.concatenate(
                [
                    normed[:, :, :, pl.ds(pl.multiple_of(256 * a, 256), 256)].reshape(384, 256)
                    for a in at
                ],
                axis=1,
            )
            for weight, total in (
                ([wa[a].reshape(256, 704) for a in at], gate),
                ([wb[a, :, 0].reshape(256, 704) for a in at], up),
            ):
                term = jnp.dot(
                    rows, jnp.concatenate(weight, axis=0), preferred_element_type=F32
                )
                total[...] = term if k == 0 else total[...] + term
        if name == "ffn":
            v = gate[...]
            hidden = (v / (1.0 + jnp.exp(-v)) * up[...]).astype(BF16)
            for k in range(8):
                w = wb[k, :, 1].reshape(256, 704)
                term = lax.dot_general(
                    hidden, w, (((1,), (1,)), ((), ())), preferred_element_type=F32
                )
                at = pl.ds(256 * k, 256)
                part[:, :, :, at] = term.astype(BF16).reshape(4, 2, 48, 256)
                wires.start(
                    lambda at=at: part.at[:, other, :, at],
                    lambda at=at: pin.at[:, :, at],
                    core_pair,
                    k,
                    "c",
                    0,
                )
            for k in range(8):
                wires.landed(lambda: pin.at[:, :, pl.ds(256 * k, 256)], core_pair, k, "c")

            def pair_sum(at_x, lo, hi):
                return part[at_x, c, :, lo:hi].astype(F32) + pin[at_x, :, lo:hi].astype(F32)

            def x_send(index, at_x, h, way):
                wires.start(
                    lambda: pin.at[at_x, :, cols(h)], lambda: xin.at[index], x_pair, index, way, 0
                )

            for at_x, h in ((xo, 0), (xo, 1), (xr, 1), (xl, 0)):
                half = slice(1024 * h, 1024 * h + 1024)
                pin[at_x, :, half] = pair_sum(at_x, half.start, half.stop).astype(BF16)
            x_send(0, xo, 0, "x+")
            x_send(1, xo, 1, "x-")
            x_send(2, xr, 1, "x+")
            x_send(3, xl, 0, "x-")
            near_r = pair_sum(xr, 0, 1024)
            near_l = pair_sum(xl, 1024, 2048)
            wires.landed(lambda: xin.at[0], x_pair, 0, "x+")
            pin[xr, :, 0:1024] = (near_r + xin[0].astype(F32)).astype(BF16)
            x_send(4, xr, 0, "x+")
            wires.landed(lambda: xin.at[1], x_pair, 1, "x-")
            pin[xl, :, 1024:2048] = (near_l + xin[1].astype(F32)).astype(BF16)
            x_send(5, xl, 1, "x-")
            for index, way in ((2, "x+"), (3, "x-"), (4, "x+"), (5, "x-")):
                wires.landed(lambda: xin.at[index], x_pair, index, way)
            low = pair_sum(x, 0, 1024) + xin[4].astype(F32) + xin[3].astype(F32)
            high = pair_sum(x, 1024, 2048) + xin[2].astype(F32) + xin[5].astype(F32)
            ffn_sum = jnp.concatenate([low, high], axis=1)
            stream = resid_alpha * normed[x, c].astype(F32) + 0.5 * ffn_sum
            out_ref[...] = layer_scaled(stream, gain_ref[1:2, :]).astype(BF16)

    plan(ka, kb, ga, gb, across, across2, attend, stage)
    wires.finish()


def body(
    resid_stream,
    q_latent,
    kv_latent,
    rope_key,
    doc_ids,
    q_gain,
    kv_gain,
    w_query,
    w_key,
    w_value,
    w_out,
    mix_gain,
    w_gate,
    w_up,
    w_down,
    out_gain,
):
    tok_rows = q_latent.shape[0]
    positions = lax.axis_index(SP) * tok_rows + jnp.arange(tok_rows, dtype=jnp.int32)
    cos_table, sin_table = rope_angles(positions)
    q_normed = rms_scaled(q_latent, q_gain)
    queries = jnp.dot(q_normed, w_query, preferred_element_type=jnp.float32).reshape(
        tok_rows, HEADS_DEV, NOPE + RD
    )
    kv_normed = rms_scaled(kv_latent, kv_gain)
    key_rot = rotate(rope_key.astype(jnp.float32), cos_table, sin_table).astype(jnp.bfloat16)
    slots = jnp.arange(64, dtype=jnp.int32)
    same = doc_ids[:, None] == slots[None, :]
    message = jnp.concatenate([kv_normed, key_rot, same.astype(BF16)], axis=1)
    apart = jnp.where(same | (slots >= 4)[None, :], 0.0, -1e30).astype(BF16)
    q_heads = []
    for h in range(HEADS_DEV):
        q_heads.append(
            jnp.concatenate(
                [
                    queries[:, h, :NOPE].astype(BF16),
                    rotate(queries[:, h, NOPE:], cos_table, sin_table).astype(BF16),
                    apart,
                ],
                axis=1,
            )
        )
    q_all = jnp.stack(q_heads)
    wkv = jnp.stack(
        [
            jnp.concatenate([w[:, 128 * h : 128 * h + 128] for w in (w_key, w_value)], axis=1)
            for h in range(HEADS_DEV)
        ]
    )

    any_spec = pl.BlockSpec(memory_space=pl.ANY)
    vmem_spec = pl.BlockSpec(memory_space=pltpu.VMEM)
    dma = pltpu.SemaphoreType.DMA
    vmem = pltpu.VMEM
    sizes = (12, 40, 32, 32, 12, 40, 8, 8, 8, 6)
    return pl.pallas_call(
        layer_kernel,
        out_shape=jax.ShapeDtypeStruct((48, 2048), BF16),
        in_specs=[vmem_spec] + [any_spec] * 4 + [vmem_spec] + [any_spec] * 2 + [vmem_spec],
        out_specs=vmem_spec,
        scratch_shapes=[
            vmem((2, NC, NZ, NY, A_ROWS, WIDE), BF16),
            vmem((2, NC, NZ, NY, B_ROWS, WIDE), BF16),
            vmem((NZ, NY, 64, 704), BF16),
            vmem((NZ, NY, 2, 64, 704), BF16),
            vmem((HEADS_DEV, tok_rows, 128), F32),
            vmem((HEADS_DEV, tok_rows, 128), F32),
            vmem((HEADS_DEV, tok_rows, 128), F32),
            vmem((8, 48, 256), BF16),
            vmem((8, 48, 256), BF16),
            vmem((2048, 2048), BF16),
            vmem((48, 2048), BF16),
            vmem((48, 2048), F32),
            vmem((NX, NC, 48, 2048), BF16),
            vmem((tok_rows, 704), F32),
            vmem((tok_rows, 704), F32),
            vmem((NX, NC, 48, 2048), BF16),
            vmem((NX, 48, 2048), BF16),
            vmem((6, 48, 1024), BF16),
            dma((8,)),
        ]
        + [dma((n,)) for n in sizes for _ in range(2)],
        compiler_params=pltpu.CompilerParams(
            collective_id=0, has_side_effects=True, vmem_limit_bytes=60 * 1024 * 1024
        ),
        name="whole_layer",
    )(
        q_all,
        message,
        w_gate,
        w_up,
        w_down.T,
        wkv,
        w_out,
        resid_stream,
        jnp.stack([mix_gain, out_gain]),
    )


def solution(mesh):
    split = Mesh(mesh.devices.reshape(NZ, NY, NX, NC), ("z", "y", "x", "c"))
    in_specs = (
        P(SP, None),
        P(SP, None),
        P(SP, None),
        P(SP, None),
        P(SP),
        P(),
        P(),
        P(None, TP),
        P(None, TP),
        P(None, TP),
        P(),
        P(),
        P(SP, TP),
        P(SP, TP),
        P(TP, SP),
        P(),
    )
    out_specs = P((*SP, *TP), None)
    return jax.shard_map(body, mesh=split, in_specs=in_specs, out_specs=out_specs, check_vma=False)
```

```python
import functools
import math

import jax
import jax.numpy as jnp
from jax import lax
from jax.experimental import pallas as pl
from jax.experimental.pallas import tpu as pltpu
from jax.sharding import Mesh
from jax.sharding import PartitionSpec as P

NOPE = 128
RD = 64
VD = 128
NZ, NY, NX, NC = 8, 4, 4, 2
SP = ("z", "y")
TP = ("x", "c")
MESH = pl.DeviceIdType.MESH

eps_norm = 1e-05
rope_theta = 10000.0
resid_alpha = 8.0**0.25
HEADS_DEV = 2
WIDE = 384
A_ROWS, B_ROWS = 64, 32
EXP2_SCALE = (NOPE + RD) ** (-0.5) * math.log2(math.e)
F32 = jnp.float32
BF16 = jnp.bfloat16


def rope_angles(positions):
    frequency = rope_theta ** (-jnp.arange(0, RD, 2, dtype=jnp.float32) / RD)
    angles = positions.astype(jnp.float32)[:, None] * frequency[None, :]
    return (jnp.cos(angles), jnp.sin(angles))


def rms_scaled(latent, scaling):
    widened = latent.astype(jnp.float32)
    inverse = lax.rsqrt(jnp.mean(widened * widened, axis=-1, keepdims=True) + eps_norm)
    return (widened * inverse * scaling).astype(jnp.bfloat16)


def layer_scaled(stream, scaling):
    centre = stream - jnp.mean(stream, axis=-1, keepdims=True)
    spread = jnp.mean(centre * centre, axis=-1, keepdims=True)
    return centre * lax.rsqrt(spread + eps_norm) * scaling


class Wires:
    def __init__(self, targets):
        self.targets = targets
        self.sent = []

    def copy(self, src, dst, pair, index, way):
        send, recv = pair
        return pltpu.make_async_remote_copy(
            src_ref=src(),
            dst_ref=dst(),
            send_sem=send.at[index],
            recv_sem=recv.at[index],
            device_id=self.targets[way],
            device_id_type=MESH,
        )

    def start(self, src, dst, pair, index, way, size):
        self.copy(src, dst, pair, index, way).start()
        self.sent.append((src, dst, pair, index, way))

    def landed(self, slot, pair, index, way):
        self.copy(slot, slot, pair, index, way).wait_recv()

    def finish(self, pairs):
        for item in self.sent:
            if any(item[2] is pair for pair in pairs):
                self.copy(*item).wait_send()
        self.sent = [item for item in self.sent if not any(item[2] is pair for pair in pairs)]


class Ring:
    def __init__(self, wires, pair, block, me, at, part, chunk=None):
        self.w, self.pair, self.block = wires, pair, block
        self.at, self.part, self.chunk = at, part, chunk
        self.z, self.y = me
        self.yl, self.yr, self.yo = (self.y + 3) % 4, (self.y + 1) % 4, (self.y + 2) % 4
        self.zz = [(self.z + d) % 8 for d in range(8)]

    def send(self, slot, index, way, blocks):
        self.w.start(slot, slot, self.pair, index, way, blocks * self.block)

    def got(self, slot, index, way="y+"):
        self.w.landed(slot, self.pair, index, way)


class RingYZ(Ring):
    def y1(self):
        own = lambda: self.at(self.z, self.y)
        self.send(own, 0, "y+", 1)
        self.send(own, 1, "y-", 1)

    def y2(self):
        self.got(lambda: self.at(self.z, self.yl), 0)
        self.got(lambda: self.at(self.z, self.yr), 1)
        self.send(lambda: self.part(self.z, self.yl, 0), 2, "y+", 0.5)
        self.send(lambda: self.part(self.z, self.yr, 1), 3, "y-", 0.5)

    def z1(self):
        self.got(lambda: self.part(self.z, self.yo, 0), 2)
        self.got(lambda: self.part(self.z, self.yo, 1), 3)
        self.send(lambda: self.chunk(self.z, 0, 4), 4, "z+", 4)
        self.send(lambda: self.chunk(self.z, 0, 4), 8, "z-", 4)

    def zs(self, s):
        right, left = self.zz[9 - s], self.zz[s - 1]
        self.got(lambda: self.chunk(right, 0, 4), 4 + s - 2)
        self.got(lambda: self.chunk(left, 0, 4), 8 + s - 2)
        if s < 4:
            self.send(lambda: self.chunk(right, 0, 4), 4 + s - 1, "z+", 4)
            self.send(lambda: self.chunk(left, 0, 4), 8 + s - 1, "z-", 4)
        else:
            self.send(lambda: self.chunk(right, 0, 2), 7, "z+", 2)
            self.send(lambda: self.chunk(left, 2, 4), 11, "z-", 2)

    def z5(self):
        self.got(lambda: self.chunk(self.zz[4], 0, 2), 7)
        self.got(lambda: self.chunk(self.zz[4], 2, 4), 11)


class RingZY(Ring):
    def z1(self):
        own = lambda: self.at(self.z, self.y)
        self.send(own, 0, "z+", 1)
        self.send(own, 4, "z-", 1)

    def zs(self, s):
        right, left = self.zz[9 - s], self.zz[s - 1]
        self.got(lambda: self.at(right, self.y), s - 2)
        self.got(lambda: self.at(left, self.y), 4 + s - 2)
        if s < 4:
            self.send(lambda: self.at(right, self.y), s - 1, "z+", 1)
            self.send(lambda: self.at(left, self.y), 4 + s - 1, "z-", 1)
        else:
            self.send(lambda: self.part(right, self.y, 0), 3, "z+", 0.5)
            self.send(lambda: self.part(left, self.y, 1), 7, "z-", 0.5)

    def z5(self):
        self.got(lambda: self.part(self.zz[4], self.y, 0), 3)
        self.got(lambda: self.part(self.zz[4], self.y, 1), 7)

    def y1(self, *steps):
        for d in steps:
            zz = self.zz[d]
            self.send(lambda zz=zz: self.at(zz, self.y), 8 + 4 * d, "y+", 1)
            self.send(lambda zz=zz: self.at(zz, self.y), 9 + 4 * d, "y-", 1)

    def y2(self, *steps):
        for d in steps:
            zz = self.zz[d]
            self.got(lambda zz=zz: self.at(zz, self.yl), 8 + 4 * d)
            self.got(lambda zz=zz: self.at(zz, self.yr), 9 + 4 * d)
            self.send(lambda zz=zz: self.part(zz, self.yl, 0), 10 + 4 * d, "y+", 0.5)
            self.send(lambda zz=zz: self.part(zz, self.yr, 1), 11 + 4 * d, "y-", 0.5)

    def y3(self, *steps):
        for d in steps:
            zz = self.zz[d]
            self.got(lambda zz=zz: self.part(zz, self.yo, 0), 10 + 4 * d)
            self.got(lambda zz=zz: self.part(zz, self.yo, 1), 11 + 4 * d)


def plan(ka, kb, ga, gb, across, across2, attend, stage):
    ka.y1()
    kb.z1()
    kb.y1(0)
    gb.y1(0)
    gb.z1()
    stage("query")
    ga.y1()
    kb.zs(2)
    kb.y1(7, 1)
    ka.y2()
    kb.y2(0)
    gb.zs(2)
    gb.y1(7)
    kb.zs(3)
    kb.y1(6, 2)
    kb.y2(7, 1)
    ka.z1()
    across(0, 0)
    gb.y2(0)
    kb.y3(0)
    across(1, 0)
    gb.zs(3)
    kb.zs(4)
    kb.y1(5, 3)
    gb.y1(2)
    across2(0, 0)
    kb.y2(6)
    across2(1, 0)
    kb.y2(2)
    kb.y3(7)
    across(1, 7)
    kb.y3(1)
    across(1, 1)
    ka.zs(2)
    across(0, 1, 7)

    def at_1_0():
        gb.y3(0)
        kb.y2(5, 3)
        across2(1, 7)
        ga.y2()
        gb.y1(6)
        across2(1, 1)
        gb.zs(4)
        kb.z5()
        kb.y1(4)
        across2(0, 1)

    def at_1_1():
        kb.y3(6)
        across(1, 6)
        kb.y3(2)
        across(1, 2)
        gb.y2(2)
        kb.y3(5)
        across(1, 5)
        ka.zs(3)
        across(0, 2, 6)
        kb.y3(3)
        across(1, 3)
        across2(0, 7)

    def at_2_0():
        ga.z1()
        gb.y1(5)
        gb.z5()

    def at_2_1():
        across2(1, 6)

    def at_3_0():
        across2(1, 5, 2)
        kb.y2(4)
        gb.y2(7)
        ka.zs(4)
        across(0, 3, 5)
        across2(0, 2)
        gb.y3(2)
        gb.y1(4)

    def at_3_1():
        across2(0, 6)

    def at_4_0():
        across2(1, 3)

    def at_4_1():
        kb.y3(4)
        across(1, 4)
        gb.y2(5)
        across2(0, 3)

    def at_5_0():
        gb.y3(7)

    def at_5_1():
        across2(0, 5)
        ga.zs(2)
        gb.y1(1)

    def at_6_0():
        ka.z5()
        across(0, 4)
        across2(1, 4)

    def at_7_0():
        gb.y2(4)
        gb.y3(5)
        gb.y2(6)
        across2(0, 4)

    def at_7_1():
        gb.y1(3)

    attend(
        {
            (1, 0): at_1_0,
            (1, 1): at_1_1,
            (2, 0): at_2_0,
            (2, 1): at_2_1,
            (3, 0): at_3_0,
            (3, 1): at_3_1,
            (4, 0): at_4_0,
            (4, 1): at_4_1,
            (5, 0): at_5_0,
            (5, 1): at_5_1,
            (6, 0): at_6_0,
            (7, 0): at_7_0,
            (7, 1): at_7_1,
        }
    )
    stage("heads")
    ga.zs(3)
    gb.y3(4)
    gb.y2(1)
    gb.y3(6)
    stage("mix")
    stage("norm")
    gb.y2(3)
    gb.y3(1)
    ga.zs(4)
    stage("spread")
    gb.y3(3)
    stage("spread2")
    stage("gate0")
    ga.z5()
    stage("gate1")
    stage("gate2")
    stage("gate3")
    stage("ffn")


def layer_kernel(
    kvl_ref,
    kvg_ref,
    rope_ref,
    doc_ref,
    turn_ref,
    qg_ref,
    mixg_ref,
    outg_ref,
    ql_ref,
    wq_ref,
    wk_ref,
    wv_ref,
    wg_ref,
    wu_ref,
    wd_ref,
    wo_ref,
    res_ref,
    out_ref,
    q_ref,
    docs,
    ql,
    wq,
    wk,
    wv,
    kva,
    kvb,
    wa,
    wb,
    m_ref,
    l_ref,
    acc_ref,
    att,
    heads,
    wo,
    res,
    mid,
    normed,
    gate,
    up,
    part,
    pin,
    xin,
    loc_sem,
    ka_s,
    ka_r,
    kb_s,
    kb_r,
    kp_s,
    kp_r,
    kx_s,
    kx_r,
    wa_s,
    wa_r,
    wb_s,
    wb_r,
    hd_s,
    hd_r,
    nx_s,
    nx_r,
    pp_s,
    pp_r,
    px_s,
    px_r,
):
    z, y = lax.axis_index("z"), lax.axis_index("y")
    x, c = lax.axis_index("x"), lax.axis_index("c")
    other = 1 - c
    zz = [(z + d) % 8 for d in range(8)]
    xr, xl, xo = (x + 1) % 4, (x + 3) % 4, (x + 2) % 4

    par = x % 2
    apar = 1 - par
    own_rows = pl.multiple_of(c * 192 + par * 96, 32)
    res_rows = pl.multiple_of((x * 2 + c) * 48, 48)
    local = [
        pltpu.make_async_copy(wg_ref, wa.at[z, y], loc_sem.at[2]),
        pltpu.make_async_copy(wu_ref, wb.at[z, y, 0], loc_sem.at[3]),
        pltpu.make_async_copy(wd_ref, wb.at[z, y, 1], loc_sem.at[4]),
    ]
    query_side = [
        pltpu.make_async_copy(ql_ref, ql, loc_sem.at[0]),
        pltpu.make_async_copy(wq_ref, wq, loc_sem.at[1]),
        pltpu.make_async_copy(wk_ref, wk, loc_sem.at[7]),
        pltpu.make_async_copy(wv_ref, wv, loc_sem.at[8]),
    ]
    later = [
        pltpu.make_async_copy(wo_ref, wo, loc_sem.at[5]),
        pltpu.make_async_copy(res_ref.at[pl.ds(res_rows, 48)], res, loc_sem.at[6]),
    ]
    for copy in local + query_side + later:
        copy.start()

    targets = {
        "z+": {"z": zz[1]},
        "z-": {"z": zz[7]},
        "y+": {"y": (y + 1) % 4},
        "y-": {"y": (y + 3) % 4},
        "c": {"c": other},
    }
    for dx in range(4):
        for dc in range(2):
            if dx or dc:
                targets[dx, dc] = {"x": (x + dx) % 4, "c": (c + dc) % 2}
    targets["x+"], targets["x-"] = targets[1, 0], targets[3, 0]
    barrier = pltpu.get_barrier_semaphore()
    greeted = ["z+", "z-", "y+", "y-"] + [k for k in targets if isinstance(k, tuple)]
    for way in greeted:
        pl.semaphore_signal(barrier, inc=1, device_id=targets[way], device_id_type=MESH)

    m_ref[...] = jnp.full(m_ref.shape, -1e30, F32)
    l_ref[...] = jnp.zeros(l_ref.shape, F32)
    acc_ref[...] = jnp.zeros(acc_ref.shape, F32)

    lane = lax.broadcasted_iota(jnp.int32, (384, 128), 1)
    docs[...] = jnp.transpose(jnp.broadcast_to(doc_ref[...].astype(F32), (128, 384)))
    own = pl.ds(own_rows, 96)
    own_lane = lane[:96]
    latent = rms_scaled(kvl_ref[own, :], kvg_ref[...])
    rope = rope_ref[own, :].astype(F32)
    turned = rope * turn_ref[0, own, :] + pltpu.roll(rope, 32, 1) * turn_ref[1, own, :]
    same = docs[own, :] == (own_lane - 64).astype(F32)
    extra = jnp.where(own_lane < 64, turned, jnp.where(same, 1.0, 0.0)).astype(BF16)
    for keys, rows in ((kva, slice(0, A_ROWS)), (kvb, slice(A_ROWS, A_ROWS + B_ROWS))):
        keys[par, c, z, y, :, 0:256] = latent[rows]
        keys[par, c, z, y, :, 256:384] = extra[rows]
    for copy in local:
        copy.wait()
    pl.semaphore_wait(barrier, len(greeted))

    wires = Wires(targets)
    me = (z, y)
    row_bytes, w_bytes = WIDE * 2, 64 * 768 * 2
    ka = RingYZ(
        wires,
        (ka_s, ka_r),
        A_ROWS * row_bytes,
        me,
        lambda a, b: kva.at[par, c, a, b],
        lambda a, b, h: kva.at[par, c, a, b, pl.ds(32 * h, 32)],
        lambda a, lo, hi: kva.at[par, c, a, pl.ds(lo, hi - lo)],
    )
    kb = RingZY(
        wires,
        (kb_s, kb_r),
        B_ROWS * row_bytes,
        me,
        lambda a, b: kvb.at[par, c, a, b],
        lambda a, b, h: kvb.at[par, c, a, b, pl.ds(16 * h, 16)],
    )
    ga = RingYZ(
        wires,
        (wa_s, wa_r),
        w_bytes,
        me,
        lambda a, b: wa.at[a, b],
        lambda a, b, h: wa.at[a, b, pl.ds(32 * h, 32)],
        lambda a, lo, hi: wa.at[a, pl.ds(lo, hi - lo)],
    )
    gb = RingZY(
        wires,
        (wb_s, wb_r),
        2 * w_bytes,
        me,
        lambda a, b: wb.at[a, b],
        lambda a, b, h: wb.at[a, b, h],
    )

    keys_of = (kva, kvb)
    core_keys, x_keys = (kp_s, kp_r), (kx_s, kx_r)

    def pair_with(color, d, theirs):
        own = apar if theirs else par
        slot = lambda: keys_of[color].at[own, c, zz[d]]
        wires.start(slot, slot, core_keys, 16 * theirs + 8 * color + d, "c", 0)

    def across(color, *steps):
        for d in steps:
            for h, way in ((0, "x+"), (1, "x-")):
                slot = lambda d=d, h=h: keys_of[color].at[par, c, zz[d], pl.ds(2 * h, 2)]
                wires.start(slot, slot, x_keys, 16 * h + 8 * color + d, way, 0)
            pair_with(color, d, 0)

    def across2(color, *steps):
        for d in steps:
            for h, way in ((0, "x+"), (1, "x-")):
                slot = lambda: keys_of[color].at[apar, c, zz[d], pl.ds(2 * h, 2)]
                wires.landed(slot, x_keys, 16 * h + 8 * color + d, way)
            pair_with(color, d, 1)

    def attend_unit(u, h):
        d = jnp.where(u % 2 == 1, (u + 1) // 2, (8 - u // 2) % 8)
        at_z = (z + d) % 8
        if h == 0:
            for theirs, own in ((0, par), (1, apar)):
                for color, keys in enumerate(keys_of):
                    wires.landed(
                        lambda: keys.at[own, other, at_z],
                        core_keys,
                        16 * theirs + 8 * color + d,
                        "c",
                    )
        rows = jnp.concatenate(
            [kva[:, :, at_z].reshape(1024, WIDE), kvb[:, :, at_z].reshape(512, WIDE)], axis=0
        )
        extra = rows[:, 256:384]
        cols_h = slice(128 * h, 128 * h + 128)
        wkv = jnp.concatenate([wk[:, cols_h], wv[:, cols_h]], axis=1)
        both = jnp.dot(rows[:, :256], wkv, preferred_element_type=F32).astype(BF16)
        keys = jnp.concatenate([both[:, :128], extra], axis=1)
        vals = both[:, 128:]
        s = lax.dot_general(
            q_ref[h], keys, (((1,), (1,)), ((), ())), preferred_element_type=F32
        )
        top_old = m_ref[h]
        top = jnp.maximum(top_old, jnp.max(s, axis=1, keepdims=True))
        factor = jnp.exp2((top_old - top) * EXP2_SCALE)
        p = jnp.exp2((s - jnp.concatenate([top] * 12, axis=1)) * EXP2_SCALE)
        total = p[:, :128]
        for k in range(1, 12):
            total = total + p[:, 128 * k : 128 * k + 128]
        m_ref[h] = top
        l_ref[h] = l_ref[h] * factor + total
        acc_ref[h] = acc_ref[h] * factor + jnp.dot(
            p.astype(BF16), vals, preferred_element_type=F32
        )

    def attend(events):
        def step(u, carry):
            for h in range(HEADS_DEV):
                for (k, at_h), event in events.items():
                    if at_h == h:
                        pl.when(u == k)(event)
                attend_unit(u, h)
            return carry

        lax.fori_loop(0, 8, step, 0)

    heads_pair, norm_pair = (hd_s, hd_r), (nx_s, nx_r)
    core_pair, x_pair = (pp_s, pp_r), (px_s, px_r)
    cols = lambda h: pl.ds(1024 * h, 1024)

    def pass_on(slot, index):
        wires.start(slot, slot, norm_pair, index, "c", 0)

    def stage(name):
        if name == "query":
            for copy in query_side:
                copy.wait()
            every = jnp.dot(
                rms_scaled(ql[...], qg_ref[...]), wq[...], preferred_element_type=F32
            )
            first, mixed, last = every[:, :128], every[:, 128:256], every[:, 256:384]
            last = pltpu.roll(last, 64, 1)
            second = jnp.where(lane < 64, pltpu.roll(mixed, 64, 1), last)
            same = docs[...] == (lane - 64).astype(F32)
            apart = jnp.where(same | (lane >= 68), 0.0, -1e30)
            for h, (plain, rotary) in enumerate(((first, mixed), (second, last))):
                swapped = jnp.where(lane < 32, pltpu.roll(rotary, 96, 1), pltpu.roll(rotary, 32, 1))
                turned = rotary * turn_ref[0] + swapped * turn_ref[1]
                q_ref[h, :, 0:128] = plain.astype(BF16)
                q_ref[h, :, 128:256] = jnp.where(lane < 64, turned, apart).astype(BF16)
        if name == "heads":
            for h in range(HEADS_DEV):
                denom = jnp.sum(l_ref[h], axis=1, keepdims=True)
                done = (acc_ref[h] / denom).astype(BF16)
                att[:, :, 128 * h : 128 * h + 128] = done.reshape(8, 48, 128)
            for dx in range(4):
                for dc in range(2):
                    if dx or dc:
                        there = (x + dx) % 4 * 2 + (c + dc) % 2
                        wires.start(
                            lambda there=there: att.at[there],
                            lambda: heads.at[x * 2 + c],
                            heads_pair,
                            2 * dx + dc,
                            (dx, dc),
                            0,
                        )
            heads[x * 2 + c] = att[x * 2 + c]
        if name == "mix":
            for dx in range(4):
                for dc in range(2):
                    if dx or dc:
                        there = (x - dx + 4) % 4 * 2 + (c + dc) % 2
                        wires.landed(
                            lambda: heads.at[there], heads_pair, 2 * dx + dc, (dx, dc)
                        )
            for copy in later:
                copy.wait()
            rows = jnp.concatenate([heads[j] for j in range(8)], axis=1)

            def mix(n, carry):
                at = pl.ds(pl.multiple_of(n * 256, 256), 256)
                mid[:, at] = jnp.dot(rows, wo[:, at], preferred_element_type=F32)
                return carry

            lax.fori_loop(0, 8, mix, 0)
        if name == "norm":
            stream = resid_alpha * res[...].astype(F32) + mid[...]
            normed[x, c] = layer_scaled(stream, mixg_ref[...]).astype(BF16)
            own = lambda: normed.at[x, c]
            for index, h, way in ((0, 0, "x+"), (1, 1, "x-"), (8, 1, "x+"), (9, 0, "x-")):
                slot = lambda h=h: normed.at[x, c, :, cols(h)]
                wires.start(slot, slot, norm_pair, index, way, 0)
            pass_on(own, 4)
        if name == "spread":
            wires.finish((ka.pair, kb.pair, x_keys, core_keys, heads_pair))
            slot = lambda: normed.at[xl, c, :, cols(0)]
            wires.landed(slot, norm_pair, 0, "x+")
            wires.start(slot, slot, norm_pair, 2, "x+", 0)
            slot_r = lambda: normed.at[xr, c, :, cols(1)]
            wires.landed(slot_r, norm_pair, 1, "x-")
            wires.start(slot_r, slot_r, norm_pair, 3, "x-", 0)
            wires.landed(lambda: normed.at[xl, c, :, cols(1)], norm_pair, 8, "x+")
            wires.landed(lambda: normed.at[xr, c, :, cols(0)], norm_pair, 9, "x-")
            pass_on(lambda: normed.at[xl, c], 5)
            pass_on(lambda: normed.at[xr, c], 6)
        if name == "spread2":
            wires.landed(lambda: normed.at[xo, c, :, cols(0)], norm_pair, 2, "x+")
            wires.landed(lambda: normed.at[xo, c, :, cols(1)], norm_pair, 3, "x-")
            pass_on(lambda: normed.at[xo, c], 7)
            for index, at in ((4, x), (5, xl), (6, xr), (7, xo)):
                wires.landed(lambda: normed.at[at, other], norm_pair, index, "c")
        if name[:4] == "gate":
            k = int(name[4:])
            near, far = ((0, 1), (7, 2), (6, 3), (5, 4))[k]
            at = [zz[near], zz[far]]
            rows = jnp.concatenate(
                [
                    normed[:, :, :, pl.ds(pl.multiple_of(256 * a, 256), 256)].reshape(384, 256)
                    for a in at
                ],
                axis=1,
            )
            for weight, total in (
                ([wa[a].reshape(256, 704) for a in at], gate),
                ([wb[a, :, 0].reshape(256, 704) for a in at], up),
            ):
                term = jnp.dot(
                    rows, jnp.concatenate(weight, axis=0), preferred_element_type=F32
                )
                total[...] = term if k == 0 else total[...] + term
        if name == "ffn":
            v = gate[...]
            hidden = (v / (1.0 + jnp.exp(-v)) * up[...]).astype(BF16)
            for k in range(8):
                w = wb[k, :, 1].reshape(256, 704)
                term = lax.dot_general(
                    hidden, w, (((1,), (1,)), ((), ())), preferred_element_type=F32
                )
                at = pl.ds(256 * k, 256)
                part[:, :, :, at] = term.astype(BF16).reshape(4, 2, 48, 256)
                wires.start(
                    lambda at=at: part.at[:, other, :, at],
                    lambda at=at: pin.at[:, :, at],
                    core_pair,
                    k,
                    "c",
                    0,
                )
            for k in range(8):
                wires.landed(lambda: pin.at[:, :, pl.ds(256 * k, 256)], core_pair, k, "c")

            def pair_sum(at_x, lo, hi):
                return part[at_x, c, :, lo:hi].astype(F32) + pin[at_x, :, lo:hi].astype(F32)

            def x_send(index, at_x, h, way):
                wires.start(
                    lambda: pin.at[at_x, :, cols(h)], lambda: xin.at[index], x_pair, index, way, 0
                )

            for at_x, h in ((xo, 0), (xo, 1), (xr, 1), (xl, 0)):
                half = slice(1024 * h, 1024 * h + 1024)
                pin[at_x, :, half] = pair_sum(at_x, half.start, half.stop).astype(BF16)
            x_send(0, xo, 0, "x+")
            x_send(1, xo, 1, "x-")
            x_send(2, xr, 1, "x+")
            x_send(3, xl, 0, "x-")
            near_r = pair_sum(xr, 0, 1024)
            near_l = pair_sum(xl, 1024, 2048)
            wires.landed(lambda: xin.at[0], x_pair, 0, "x+")
            pin[xr, :, 0:1024] = (near_r + xin[0].astype(F32)).astype(BF16)
            x_send(4, xr, 0, "x+")
            wires.landed(lambda: xin.at[1], x_pair, 1, "x-")
            pin[xl, :, 1024:2048] = (near_l + xin[1].astype(F32)).astype(BF16)
            x_send(5, xl, 1, "x-")
            wires.finish((ga.pair, gb.pair, norm_pair, core_pair))
            for index, way in ((2, "x+"), (3, "x-"), (4, "x+"), (5, "x-")):
                wires.landed(lambda: xin.at[index], x_pair, index, way)
            low = pair_sum(x, 0, 1024) + xin[4].astype(F32) + xin[3].astype(F32)
            high = pair_sum(x, 1024, 2048) + xin[2].astype(F32) + xin[5].astype(F32)
            ffn_sum = jnp.concatenate([low, high], axis=1)
            stream = resid_alpha * normed[x, c].astype(F32) + 0.5 * ffn_sum
            out_ref[...] = layer_scaled(stream, outg_ref[...]).astype(BF16)

    plan(ka, kb, ga, gb, across, across2, attend, stage)
    wires.finish((x_pair,))


def body(
    resid_stream,
    q_latent,
    kv_latent,
    rope_key,
    doc_ids,
    q_gain,
    kv_gain,
    w_query,
    w_key,
    w_value,
    w_out,
    mix_gain,
    w_gate,
    w_up,
    w_down,
    out_gain,
):
    tok_rows = q_latent.shape[0]
    positions = lax.axis_index(SP) * tok_rows + jnp.arange(tok_rows, dtype=jnp.int32)
    cos_table, sin_table = rope_angles(positions)
    turn = jnp.stack(
        [
            jnp.concatenate([cos_table] * 4, axis=1),
            jnp.concatenate([-sin_table, sin_table] * 2, axis=1),
        ]
    )
    any_spec = pl.BlockSpec(memory_space=pl.ANY)
    vmem_spec = pl.BlockSpec(memory_space=pltpu.VMEM)
    dma = pltpu.SemaphoreType.DMA
    vmem = pltpu.VMEM
    sizes = (12, 40, 32, 32, 12, 40, 8, 10, 8, 6)
    return pl.pallas_call(
        layer_kernel,
        out_shape=jax.ShapeDtypeStruct((48, 2048), BF16),
        in_specs=[vmem_spec] * 8 + [any_spec] * 9,
        out_specs=vmem_spec,
        scratch_shapes=[
            vmem((HEADS_DEV, tok_rows, 256), BF16),
            vmem((tok_rows, 128), F32),
            vmem(q_latent.shape, BF16),
            vmem(w_query.shape, BF16),
            vmem(w_key.shape, BF16),
            vmem(w_value.shape, BF16),
            vmem((2, NC, NZ, NY, A_ROWS, WIDE), BF16),
            vmem((2, NC, NZ, NY, B_ROWS, WIDE), BF16),
            vmem((NZ, NY, 64, 704), BF16),
            vmem((NZ, NY, 2, 64, 704), BF16),
            vmem((HEADS_DEV, tok_rows, 128), F32),
            vmem((HEADS_DEV, tok_rows, 128), F32),
            vmem((HEADS_DEV, tok_rows, 128), F32),
            vmem((8, 48, 256), BF16),
            vmem((8, 48, 256), BF16),
            vmem((2048, 2048), BF16),
            vmem((48, 2048), BF16),
            vmem((48, 2048), F32),
            vmem((NX, NC, 48, 2048), BF16),
            vmem((tok_rows, 704), F32),
            vmem((tok_rows, 704), F32),
            vmem((NX, NC, 48, 2048), BF16),
            vmem((NX, 48, 2048), BF16),
            vmem((6, 48, 1024), BF16),
            dma((9,)),
        ]
        + [dma((n,)) for n in sizes for _ in range(2)],
        compiler_params=pltpu.CompilerParams(
            collective_id=0, has_side_effects=True, vmem_limit_bytes=60 * 1024 * 1024
        ),
        name="whole_layer",
    )(
        kv_latent,
        kv_gain.reshape(1, -1),
        jnp.concatenate([rope_key, rope_key], axis=1),
        doc_ids.reshape(1, -1),
        turn,
        q_gain.reshape(1, -1),
        mix_gain.reshape(1, -1),
        out_gain.reshape(1, -1),
        q_latent,
        w_query,
        w_key,
        w_value,
        w_gate,
        w_up,
        w_down.T,
        w_out,
        resid_stream,
    )


def solution(mesh):
    split = Mesh(mesh.devices.reshape(NZ, NY, NX, NC), ("z", "y", "x", "c"))
    in_specs = (
        P(SP, None),
        P(SP, None),
        P(SP, None),
        P(SP, None),
        P(SP),
        P(),
        P(),
        P(None, TP),
        P(None, TP),
        P(None, TP),
        P(),
        P(),
        P(SP, TP),
        P(SP, TP),
        P(TP, SP),
        P(),
    )
    out_specs = P((*SP, *TP), None)
    return jax.shard_map(body, mesh=split, in_specs=in_specs, out_specs=out_specs, check_vma=False)
```

```python
import functools
import math

import jax
import jax.numpy as jnp
from jax import lax
from jax.experimental import pallas as pl
from jax.experimental.pallas import tpu as pltpu
from jax.sharding import Mesh
from jax.sharding import PartitionSpec as P

NOPE = 128
RD = 64
VD = 128
NZ, NY, NX, NC = 8, 4, 4, 2
SP = ("z", "y")
TP = ("x", "c")
MESH = pl.DeviceIdType.MESH

eps_norm = 1e-05
rope_theta = 10000.0
resid_alpha = 8.0**0.25
HEADS_DEV = 2
WIDE = 384
A_ROWS, B_ROWS = 64, 32
EXP2_SCALE = (NOPE + RD) ** (-0.5) * math.log2(math.e)
F32 = jnp.float32
BF16 = jnp.bfloat16


def rope_angles(positions):
    lane = jnp.arange(128, dtype=jnp.int32)
    frequency = rope_theta ** (-2.0 * (lane % 32).astype(jnp.float32) / RD)
    angles = positions.astype(jnp.float32)[:, None] * frequency[None, :]
    sign = jnp.where(lane % 64 < 32, -1.0, 1.0)
    return (jnp.cos(angles), jnp.sin(angles) * sign[None, :])


def rms_scaled(latent, scaling):
    widened = latent.astype(jnp.float32)
    inverse = lax.rsqrt(jnp.mean(widened * widened, axis=-1, keepdims=True) + eps_norm)
    return (widened * inverse * scaling).astype(jnp.bfloat16)


def layer_scaled(stream, scaling):
    centre = stream - jnp.mean(stream, axis=-1, keepdims=True)
    spread = jnp.mean(centre * centre, axis=-1, keepdims=True)
    return centre * lax.rsqrt(spread + eps_norm) * scaling


class Wires:
    def __init__(self, targets):
        self.targets = targets

    def copy(self, src, dst, pair, index, way, out=0):
        send, recv = pair
        return pltpu.make_async_remote_copy(
            src_ref=src(),
            dst_ref=dst(),
            send_sem=send.at[out],
            recv_sem=recv.at[index],
            device_id=self.targets[way],
            device_id_type=MESH,
        )

    def start(self, src, dst, pair, index, way, size, out=0):
        self.copy(src, dst, pair, index, way, out).start()

    def landed(self, slot, pair, index, way):
        self.copy(slot, slot, pair, index, way).wait_recv()

    def left(self, pair, out, as_many):
        region = lambda: as_many
        self.copy(region, region, pair, 0, "c", out).wait_send()


class Ring:
    def __init__(self, wires, pair, block, me, at, part, chunk=None):
        self.w, self.pair, self.block = wires, pair, block
        self.at, self.part, self.chunk = at, part, chunk
        self.z, self.y = me
        self.yl, self.yr, self.yo = (self.y + 3) % 4, (self.y + 1) % 4, (self.y + 2) % 4
        self.zz = [(self.z + d) % 8 for d in range(8)]

    def send(self, slot, index, way, blocks):
        self.w.start(slot, slot, self.pair, index, way, blocks * self.block, int(way[0] == "z"))

    def got(self, slot, index, way="y+"):
        self.w.landed(slot, self.pair, index, way)


class RingYZ(Ring):
    def y1(self):
        own = lambda: self.at(self.z, self.y)
        self.send(own, 0, "y+", 1)
        self.send(own, 1, "y-", 1)

    def y2(self):
        self.got(lambda: self.at(self.z, self.yl), 0)
        self.got(lambda: self.at(self.z, self.yr), 1)
        self.send(lambda: self.part(self.z, self.yl, 0), 2, "y+", 0.5)
        self.send(lambda: self.part(self.z, self.yr, 1), 3, "y-", 0.5)

    def z1(self):
        self.got(lambda: self.part(self.z, self.yo, 0), 2)
        self.got(lambda: self.part(self.z, self.yo, 1), 3)
        for h in range(2):
            self.send(lambda h=h: self.half(self.z, h), 4 + 4 * h, "z+", 2)
            self.send(lambda h=h: self.half(self.z, h), 12 + 4 * h, "z-", 2)

    def half(self, a, h):
        return self.chunk(a, 2 * h, 2 * h + 2)

    def zs(self, s, h):
        right, left = self.zz[9 - s], self.zz[s - 1]
        self.got(lambda: self.half(right, h), 4 + 4 * h + s - 2)
        self.got(lambda: self.half(left, h), 12 + 4 * h + s - 2)
        if s < 4 or h == 0:
            self.send(lambda: self.half(right, h), 4 + 4 * h + s - 1, "z+", 2)
        if s < 4 or h == 1:
            self.send(lambda: self.half(left, h), 12 + 4 * h + s - 1, "z-", 2)

    def z5(self):
        self.got(lambda: self.half(self.zz[4], 0), 7)
        self.got(lambda: self.half(self.zz[4], 1), 19)

    def left(self, whole):
        self.w.left(self.pair, 0, whole.at[0, pl.ds(0, 3)])
        self.w.left(self.pair, 1, whole.at[pl.ds(0, 7)])


class RingZY(Ring):
    def z1(self):
        own = lambda: self.at(self.z, self.y)
        self.send(own, 0, "z+", 1)
        self.send(own, 4, "z-", 1)

    def zs(self, s):
        right, left = self.zz[9 - s], self.zz[s - 1]
        self.got(lambda: self.at(right, self.y), s - 2)
        self.got(lambda: self.at(left, self.y), 4 + s - 2)
        if s < 4:
            self.send(lambda: self.at(right, self.y), s - 1, "z+", 1)
            self.send(lambda: self.at(left, self.y), 4 + s - 1, "z-", 1)
        else:
            self.send(lambda: self.part(right, self.y, 0), 3, "z+", 0.5)
            self.send(lambda: self.part(left, self.y, 1), 7, "z-", 0.5)

    def z5(self):
        self.got(lambda: self.part(self.zz[4], self.y, 0), 3)
        self.got(lambda: self.part(self.zz[4], self.y, 1), 7)

    def y1(self, *steps):
        for d in steps:
            zz = self.zz[d]
            self.send(lambda zz=zz: self.at(zz, self.y), 8 + 4 * d, "y+", 1)
            self.send(lambda zz=zz: self.at(zz, self.y), 9 + 4 * d, "y-", 1)

    def y2(self, *steps):
        for d in steps:
            zz = self.zz[d]
            self.got(lambda zz=zz: self.at(zz, self.yl), 8 + 4 * d)
            self.got(lambda zz=zz: self.at(zz, self.yr), 9 + 4 * d)
            self.send(lambda zz=zz: self.part(zz, self.yl, 0), 10 + 4 * d, "y+", 0.5)
            self.send(lambda zz=zz: self.part(zz, self.yr, 1), 11 + 4 * d, "y-", 0.5)

    def y3(self, *steps):
        for d in steps:
            zz = self.zz[d]
            self.got(lambda zz=zz: self.part(zz, self.yo, 0), 10 + 4 * d)
            self.got(lambda zz=zz: self.part(zz, self.yo, 1), 11 + 4 * d)

    def left(self, whole):
        self.w.left(self.pair, 0, whole.at[pl.ds(0, 6)])
        self.w.left(self.pair, 1, whole.at[pl.ds(0, 7), 0])


def plan(ka, kb, ga, gb, across, across2, attend, stage):
    ka.y1()
    kb.z1()
    kb.y1(0)
    gb.z1()
    stage("query")
    ga.y1()
    kb.zs(2)
    kb.y1(1, 7)
    ka.y2()
    kb.y2(0)
    gb.y1(0)
    gb.zs(2)
    kb.y2(1)
    kb.zs(3)
    kb.y1(6, 2)
    kb.y2(7)
    ka.z1()
    across(0, 0)
    kb.y3(0)
    across(1, 0)
    gb.y1(7)
    across2(0, 0)
    kb.y3(1)
    across(1, 1)
    kb.y2(6)
    across2(1, 0)
    kb.y2(2)
    kb.zs(4)
    kb.y1(5)
    kb.y3(7)
    across(1, 7)
    kb.y1(3)

    def at_0_1():
        ka.zs(2, 0)
        across2(1, 1)

    def at_1_0():
        ga.y2()
        gb.zs(3)
        gb.y2(0)
        across2(1, 7)
        ka.zs(2, 1)
        across(0, 1, 7)
        kb.z5()
        kb.y1(4)
        kb.y3(6)
        across(1, 6)
        kb.y3(2)
        across(1, 2)
        kb.y2(5, 3)
        ka.zs(3, 0)
        gb.y1(6)
        across2(0, 1)
        gb.y3(0)
        kb.y2(4)
        kb.y3(5)
        across(1, 5)

    def at_1_1():
        across2(0, 7)
        kb.y3(3)
        across(1, 3)
        gb.y1(1)

    def at_2_0():
        across2(1, 6)
        ka.zs(3, 1)
        across(0, 2, 6)
        across2(1, 2)

    def at_2_1():
        across2(1, 5)
        gb.zs(4)

    def at_3_0():
        across2(1, 3)
        gb.y2(6)
        kb.y3(4)
        across(1, 4)
        ka.zs(4, 0)
        ka.zs(4, 1)
        across(0, 3)
        across2(0, 2)
        across(0, 5)
        gb.y1(3)
        ga.z1()

    def at_3_1():
        gb.z5()
        across2(0, 6)

    def at_4_0():
        gb.y3(6)
        across2(1, 4)
        gb.y1(4)
        ka.z5()
        across(0, 4)

    def at_4_1():
        across2(0, 3)

    def at_5_1():
        across2(0, 5)
        gb.y1(5)

    def at_6_0():
        ga.zs(2, 0)
        across2(0, 4)

    def at_7_0():
        gb.y2(1)

    def at_7_1():
        ga.zs(2, 1)

    attend(
        {
            (0, 1): at_0_1,
            (1, 0): at_1_0,
            (1, 1): at_1_1,
            (2, 0): at_2_0,
            (2, 1): at_2_1,
            (3, 0): at_3_0,
            (3, 1): at_3_1,
            (4, 0): at_4_0,
            (4, 1): at_4_1,
            (5, 1): at_5_1,
            (6, 0): at_6_0,
            (7, 0): at_7_0,
            (7, 1): at_7_1,
        }
    )
    gb.y2(4)
    stage("heads")
    gb.y2(5)
    ga.zs(3, 0)
    gb.y3(1)
    gb.y2(3)
    gb.y3(4)
    gb.y1(2)
    stage("mix")
    ga.zs(3, 1)
    gb.y3(5)
    stage("norm")
    ga.zs(4, 0)
    gb.y3(3)
    gb.y2(7)
    stage("spread")
    gb.y2(2)
    ga.zs(4, 1)
    gb.y3(7)
    stage("spread2")
    gb.y3(2)
    stage("gate0")
    stage("gate1")
    stage("gate2")
    ga.z5()
    stage("gate3")
    stage("ffn")


def layer_kernel(
    kvl_ref,
    kvg_ref,
    rope_ref,
    doc_ref,
    cos_ref,
    sin_ref,
    qg_ref,
    mixg_ref,
    outg_ref,
    ql_ref,
    wq_ref,
    wk_ref,
    wv_ref,
    wg_ref,
    wu_ref,
    wd_ref,
    wo_ref,
    res_ref,
    out_ref,
    q_ref,
    docs,
    ropes,
    ql,
    wq,
    wk,
    wv,
    kva,
    kvb,
    wa,
    wb,
    m_ref,
    l_ref,
    acc_ref,
    att,
    heads,
    wo,
    res,
    mid,
    normed,
    gate,
    up,
    part,
    pin,
    xin,
    loc_sem,
    ka_s,
    ka_r,
    kb_s,
    kb_r,
    kp_s,
    kp_r,
    kx_s,
    kx_r,
    wa_s,
    wa_r,
    wb_s,
    wb_r,
    hd_s,
    hd_r,
    nx_s,
    nx_r,
    pp_s,
    pp_r,
    px_s,
    px_r,
):
    z, y = lax.axis_index("z"), lax.axis_index("y")
    x, c = lax.axis_index("x"), lax.axis_index("c")
    other = 1 - c
    zz = [(z + d) % 8 for d in range(8)]
    xr, xl, xo = (x + 1) % 4, (x + 3) % 4, (x + 2) % 4

    par = x % 2
    apar = 1 - par
    own_rows = pl.multiple_of(c * 192 + par * 96, 32)
    res_rows = pl.multiple_of((x * 2 + c) * 48, 48)
    local = [
        pltpu.make_async_copy(wg_ref, wa.at[z, y], loc_sem.at[2]),
        pltpu.make_async_copy(wu_ref, wb.at[z, y, 0], loc_sem.at[3]),
        pltpu.make_async_copy(wd_ref, wb.at[z, y, 1], loc_sem.at[4]),
    ]
    query_side = [
        pltpu.make_async_copy(ql_ref, ql, loc_sem.at[0]),
        pltpu.make_async_copy(wq_ref, wq, loc_sem.at[1]),
        pltpu.make_async_copy(wk_ref, wk, loc_sem.at[7]),
        pltpu.make_async_copy(wv_ref, wv, loc_sem.at[8]),
    ]
    later = [
        pltpu.make_async_copy(wo_ref, wo, loc_sem.at[5]),
        pltpu.make_async_copy(res_ref.at[pl.ds(res_rows, 48)], res, loc_sem.at[6]),
    ]
    for copy in local + query_side + later:
        copy.start()

    targets = {
        "z+": {"z": zz[1]},
        "z-": {"z": zz[7]},
        "y+": {"y": (y + 1) % 4},
        "y-": {"y": (y + 3) % 4},
        "c": {"c": other},
    }
    for dx in range(4):
        for dc in range(2):
            if dx or dc:
                targets[dx, dc] = {"x": (x + dx) % 4, "c": (c + dc) % 2}
    targets["x+"], targets["x-"] = targets[1, 0], targets[3, 0]
    barrier = pltpu.get_barrier_semaphore()
    greeted = ["z+", "z-", "y+", "y-"] + [k for k in targets if isinstance(k, tuple)]
    for way in greeted:
        pl.semaphore_signal(barrier, inc=1, device_id=targets[way], device_id_type=MESH)

    m_ref[...] = jnp.full(m_ref.shape, -1e30, F32)
    l_ref[...] = jnp.zeros(l_ref.shape, F32)
    acc_ref[...] = jnp.zeros(acc_ref.shape, F32)

    lane = lax.broadcasted_iota(jnp.int32, (384, 128), 1)
    doc_row = doc_ref[...].reshape(1, 384).astype(F32)
    docs[...] = jnp.transpose(jnp.broadcast_to(doc_row, (128, 384)))
    rope_rows = rope_ref[...].astype(F32)
    ropes[...] = jnp.transpose(jnp.concatenate([rope_rows, rope_rows], axis=0))
    own = pl.ds(own_rows, 96)
    own_lane = lane[:96]
    latent = rms_scaled(kvl_ref[own, :], kvg_ref[...])
    rope = ropes[own, :]
    turned = rope * cos_ref[own, :] + pltpu.roll(rope, 32, 1) * sin_ref[own, :]
    same = docs[own, :] == (own_lane - 64).astype(F32)
    extra = jnp.where(own_lane < 64, turned, jnp.where(same, 1.0, 0.0)).astype(BF16)
    for keys, rows in ((kva, slice(0, A_ROWS)), (kvb, slice(A_ROWS, A_ROWS + B_ROWS))):
        keys[par, c, z, y, :, 0:256] = latent[rows]
        keys[par, c, z, y, :, 256:384] = extra[rows]
    for copy in local:
        copy.wait()
    pl.semaphore_wait(barrier, len(greeted))

    wires = Wires(targets)
    me = (z, y)
    row_bytes, w_bytes = WIDE * 2, 64 * 768 * 2
    ka = RingYZ(
        wires,
        (ka_s, ka_r),
        A_ROWS * row_bytes,
        me,
        lambda a, b: kva.at[par, c, a, b],
        lambda a, b, h: kva.at[par, c, a, b, pl.ds(32 * h, 32)],
        lambda a, lo, hi: kva.at[par, c, a, pl.ds(lo, hi - lo)],
    )
    kb = RingZY(
        wires,
        (kb_s, kb_r),
        B_ROWS * row_bytes,
        me,
        lambda a, b: kvb.at[par, c, a, b],
        lambda a, b, h: kvb.at[par, c, a, b, pl.ds(16 * h, 16)],
    )
    ga = RingYZ(
        wires,
        (wa_s, wa_r),
        w_bytes,
        me,
        lambda a, b: wa.at[a, b],
        lambda a, b, h: wa.at[a, b, pl.ds(32 * h, 32)],
        lambda a, lo, hi: wa.at[a, pl.ds(lo, hi - lo)],
    )
    gb = RingZY(
        wires,
        (wb_s, wb_r),
        2 * w_bytes,
        me,
        lambda a, b: wb.at[a, b],
        lambda a, b, h: wb.at[a, b, h],
    )

    keys_of = (kva, kvb)
    core_keys, x_keys = (kp_s, kp_r), (kx_s, kx_r)

    def pair_with(color, d, theirs):
        own = apar if theirs else par
        slot = lambda: keys_of[color].at[own, c, zz[d]]
        wires.start(slot, slot, core_keys, 16 * theirs + 8 * color + d, "c", 0, 2 * theirs + color)

    def across(color, *steps):
        for d in steps:
            for h, way in ((0, "x+"), (1, "x-")):
                slot = lambda d=d, h=h: keys_of[color].at[par, c, zz[d], pl.ds(2 * h, 2)]
                wires.start(slot, slot, x_keys, 16 * h + 8 * color + d, way, 0, color)
            pair_with(color, d, 0)

    def across2(color, *steps):
        for d in steps:
            for h, way in ((0, "x+"), (1, "x-")):
                slot = lambda: keys_of[color].at[apar, c, zz[d], pl.ds(2 * h, 2)]
                wires.landed(slot, x_keys, 16 * h + 8 * color + d, way)
            pair_with(color, d, 1)

    def attend_unit(u, h):
        d = jnp.where(u % 2 == 1, (u + 1) // 2, (8 - u // 2) % 8)
        at_z = (z + d) % 8
        if h == 0:
            for theirs, own in ((0, par), (1, apar)):
                for color, keys in enumerate(keys_of):
                    wires.landed(
                        lambda: keys.at[own, other, at_z],
                        core_keys,
                        16 * theirs + 8 * color + d,
                        "c",
                    )
        rows = jnp.concatenate(
            [kva[:, :, at_z].reshape(1024, WIDE), kvb[:, :, at_z].reshape(512, WIDE)], axis=0
        )
        extra = rows[:, 256:384]
        cols_h = slice(128 * h, 128 * h + 128)
        wkv = jnp.concatenate([wk[:, cols_h], wv[:, cols_h]], axis=1)
        both = jnp.dot(rows[:, :256], wkv, preferred_element_type=F32).astype(BF16)
        keys = jnp.concatenate([both[:, :128], extra], axis=1)
        vals = both[:, 128:]
        s = lax.dot_general(
            q_ref[h], keys, (((1,), (1,)), ((), ())), preferred_element_type=F32
        )
        top_old = m_ref[h]
        top = jnp.maximum(top_old, jnp.max(s, axis=1, keepdims=True))
        factor = jnp.exp2((top_old - top) * EXP2_SCALE)
        p = jnp.exp2((s - jnp.concatenate([top] * 12, axis=1)) * EXP2_SCALE)
        total = p[:, :128]
        for k in range(1, 12):
            total = total + p[:, 128 * k : 128 * k + 128]
        m_ref[h] = top
        l_ref[h] = l_ref[h] * factor + total
        acc_ref[h] = acc_ref[h] * factor + jnp.dot(
            p.astype(BF16), vals, preferred_element_type=F32
        )

    def attend(events):
        def step(u, carry):
            for h in range(HEADS_DEV):
                for (k, at_h), event in events.items():
                    if at_h == h:
                        pl.when(u == k)(event)
                attend_unit(u, h)
            return carry

        lax.fori_loop(0, 8, step, 0)

    heads_pair, norm_pair = (hd_s, hd_r), (nx_s, nx_r)
    core_pair, x_pair = (pp_s, pp_r), (px_s, px_r)
    cols = lambda h: pl.ds(1024 * h, 1024)

    def pass_on(slot, index):
        wires.start(slot, slot, norm_pair, index, "c", 0, 1)

    def stage(name):
        if name == "query":
            for copy in query_side:
                copy.wait()
            every = jnp.dot(
                rms_scaled(ql[...], qg_ref[...]), wq[...], preferred_element_type=F32
            )
            first, mixed, last = every[:, :128], every[:, 128:256], every[:, 256:384]
            last = pltpu.roll(last, 64, 1)
            second = jnp.where(lane < 64, pltpu.roll(mixed, 64, 1), last)
            same = docs[...] == (lane - 64).astype(F32)
            apart = jnp.where(same | (lane >= 68), 0.0, -1e30)
            for h, (plain, rotary) in enumerate(((first, mixed), (second, last))):
                swapped = jnp.where(lane < 32, pltpu.roll(rotary, 96, 1), pltpu.roll(rotary, 32, 1))
                turned = rotary * cos_ref[...] + swapped * sin_ref[...]
                q_ref[h, :, 0:128] = plain.astype(BF16)
                q_ref[h, :, 128:256] = jnp.where(lane < 64, turned, apart).astype(BF16)
        if name == "heads":
            for h in range(HEADS_DEV):
                denom = jnp.sum(l_ref[h], axis=1, keepdims=True)
                done = (acc_ref[h] / denom).astype(BF16)
                att[:, :, 128 * h : 128 * h + 128] = done.reshape(8, 48, 128)
            for dx in range(4):
                for dc in range(2):
                    if dx or dc:
                        there = (x + dx) % 4 * 2 + (c + dc) % 2
                        wires.start(
                            lambda there=there: att.at[there],
                            lambda: heads.at[x * 2 + c],
                            heads_pair,
                            2 * dx + dc,
                            (dx, dc),
                            0,
                        )
            heads[x * 2 + c] = att[x * 2 + c]
        if name == "mix":
            for dx in range(4):
                for dc in range(2):
                    if dx or dc:
                        there = (x - dx + 4) % 4 * 2 + (c + dc) % 2
                        wires.landed(
                            lambda: heads.at[there], heads_pair, 2 * dx + dc, (dx, dc)
                        )
            for copy in later:
                copy.wait()
            rows = jnp.concatenate([heads[j] for j in range(8)], axis=1)

            def mix(n, carry):
                at = pl.ds(pl.multiple_of(n * 256, 256), 256)
                mid[:, at] = jnp.dot(rows, wo[:, at], preferred_element_type=F32)
                return carry

            lax.fori_loop(0, 8, mix, 0)
        if name == "norm":
            stream = resid_alpha * res[...].astype(F32) + mid[...]
            normed[x, c] = layer_scaled(stream, mixg_ref[...]).astype(BF16)
            own = lambda: normed.at[x, c]
            for index, h, way in ((0, 0, "x+"), (1, 1, "x-"), (8, 1, "x+"), (9, 0, "x-")):
                slot = lambda h=h: normed.at[x, c, :, cols(h)]
                wires.start(slot, slot, norm_pair, index, way, 0)
            pass_on(own, 4)
        if name == "spread":
            ka.left(kva.at[par, c])
            kb.left(kvb.at[par, c])
            for color, keys in enumerate(keys_of):
                wires.left(x_keys, color, keys.at[par, c])
                wires.left(core_keys, color, keys.at[par, c])
                wires.left(core_keys, 2 + color, keys.at[apar, c])
            wires.left(heads_pair, 0, heads.at[pl.ds(0, 7)])
            slot = lambda: normed.at[xl, c, :, cols(0)]
            wires.landed(slot, norm_pair, 0, "x+")
            wires.start(slot, slot, norm_pair, 2, "x+", 0)
            slot_r = lambda: normed.at[xr, c, :, cols(1)]
            wires.landed(slot_r, norm_pair, 1, "x-")
            wires.start(slot_r, slot_r, norm_pair, 3, "x-", 0)
            wires.landed(lambda: normed.at[xl, c, :, cols(1)], norm_pair, 8, "x+")
            wires.landed(lambda: normed.at[xr, c, :, cols(0)], norm_pair, 9, "x-")
            pass_on(lambda: normed.at[xl, c], 5)
            pass_on(lambda: normed.at[xr, c], 6)
        if name == "spread2":
            wires.landed(lambda: normed.at[xo, c, :, cols(0)], norm_pair, 2, "x+")
            wires.landed(lambda: normed.at[xo, c, :, cols(1)], norm_pair, 3, "x-")
            pass_on(lambda: normed.at[xo, c], 7)
            for index, at in ((4, x), (5, xl), (6, xr), (7, xo)):
                wires.landed(lambda: normed.at[at, other], norm_pair, index, "c")
        if name[:4] == "gate":
            k = int(name[4:])
            near, far = ((0, 1), (7, 2), (6, 3), (5, 4))[k]
            at = [zz[near], zz[far]]
            rows = jnp.concatenate(
                [
                    normed[:, :, :, pl.ds(pl.multiple_of(256 * a, 256), 256)].reshape(384, 256)
                    for a in at
                ],
                axis=1,
            )
            for weight, total in (
                ([wa[a].reshape(256, 704) for a in at], gate),
                ([wb[a, :, 0].reshape(256, 704) for a in at], up),
            ):
                term = jnp.dot(
                    rows, jnp.concatenate(weight, axis=0), preferred_element_type=F32
                )
                total[...] = term if k == 0 else total[...] + term
        if name == "ffn":
            v = gate[...]
            hidden = (v / (1.0 + jnp.exp(-v)) * up[...]).astype(BF16)
            for k in range(8):
                w = wb[k, :, 1].reshape(256, 704)
                term = lax.dot_general(
                    hidden, w, (((1,), (1,)), ((), ())), preferred_element_type=F32
                )
                at = pl.ds(256 * k, 256)
                part[:, :, :, at] = term.astype(BF16).reshape(4, 2, 48, 256)
                wires.start(
                    lambda at=at: part.at[:, other, :, at],
                    lambda at=at: pin.at[:, :, at],
                    core_pair,
                    k,
                    "c",
                    0,
                )
            for k in range(8):
                wires.landed(lambda: pin.at[:, :, pl.ds(256 * k, 256)], core_pair, k, "c")

            def pair_sum(at_x, lo, hi):
                return part[at_x, c, :, lo:hi].astype(F32) + pin[at_x, :, lo:hi].astype(F32)

            def x_send(index, at_x, h, way):
                wires.start(
                    lambda: pin.at[at_x, :, cols(h)], lambda: xin.at[index], x_pair, index, way, 0
                )

            for at_x, h in ((xo, 0), (xo, 1), (xr, 1), (xl, 0)):
                half = slice(1024 * h, 1024 * h + 1024)
                pin[at_x, :, half] = pair_sum(at_x, half.start, half.stop).astype(BF16)
            x_send(0, xo, 0, "x+")
            x_send(1, xo, 1, "x-")
            x_send(2, xr, 1, "x+")
            x_send(3, xl, 0, "x-")
            near_r = pair_sum(xr, 0, 1024)
            near_l = pair_sum(xl, 1024, 2048)
            wires.landed(lambda: xin.at[0], x_pair, 0, "x+")
            pin[xr, :, 0:1024] = (near_r + xin[0].astype(F32)).astype(BF16)
            x_send(4, xr, 0, "x+")
            wires.landed(lambda: xin.at[1], x_pair, 1, "x-")
            pin[xl, :, 1024:2048] = (near_l + xin[1].astype(F32)).astype(BF16)
            x_send(5, xl, 1, "x-")
            ga.left(wa)
            gb.left(wb)
            wires.left(norm_pair, 0, normed.at[pl.ds(0, 3), 0])
            wires.left(norm_pair, 1, normed.at[:, 0])
            wires.left(core_pair, 0, pin)
            for index, way in ((2, "x+"), (3, "x-"), (4, "x+"), (5, "x-")):
                wires.landed(lambda: xin.at[index], x_pair, index, way)
            low = pair_sum(x, 0, 1024) + xin[4].astype(F32) + xin[3].astype(F32)
            high = pair_sum(x, 1024, 2048) + xin[2].astype(F32) + xin[5].astype(F32)
            ffn_sum = jnp.concatenate([low, high], axis=1)
            stream = resid_alpha * normed[x, c].astype(F32) + 0.5 * ffn_sum
            out_ref[...] = layer_scaled(stream, outg_ref[...]).astype(BF16)

    plan(ka, kb, ga, gb, across, across2, attend, stage)
    wires.left(x_pair, 0, xin)


def body(
    resid_stream,
    q_latent,
    kv_latent,
    rope_key,
    doc_ids,
    q_gain,
    kv_gain,
    w_query,
    w_key,
    w_value,
    w_out,
    mix_gain,
    w_gate,
    w_up,
    w_down,
    out_gain,
):
    tok_rows = q_latent.shape[0]
    positions = lax.axis_index(SP) * tok_rows + jnp.arange(tok_rows, dtype=jnp.int32)
    cos_table, sin_table = rope_angles(positions)
    any_spec = pl.BlockSpec(memory_space=pl.ANY)
    vmem_spec = pl.BlockSpec(memory_space=pltpu.VMEM)
    dma = pltpu.SemaphoreType.DMA
    vmem = pltpu.VMEM
    sizes = (2, 20, 2, 40, 4, 32, 2, 32, 2, 20, 2, 40, 1, 8, 2, 10, 1, 8, 1, 6)
    return pl.pallas_call(
        layer_kernel,
        out_shape=jax.ShapeDtypeStruct((48, 2048), BF16),
        in_specs=[vmem_spec] * 9 + [any_spec] * 9,
        out_specs=vmem_spec,
        scratch_shapes=[
            vmem((HEADS_DEV, tok_rows, 256), BF16),
            vmem((tok_rows, 128), F32),
            vmem((tok_rows, 128), F32),
            vmem(q_latent.shape, BF16),
            vmem(w_query.shape, BF16),
            vmem(w_key.shape, BF16),
            vmem(w_value.shape, BF16),
            vmem((2, NC, NZ, NY, A_ROWS, WIDE), BF16),
            vmem((2, NC, NZ, NY, B_ROWS, WIDE), BF16),
            vmem((NZ, NY, 64, 704), BF16),
            vmem((NZ, NY, 2, 64, 704), BF16),
            vmem((HEADS_DEV, tok_rows, 128), F32),
            vmem((HEADS_DEV, tok_rows, 128), F32),
            vmem((HEADS_DEV, tok_rows, 128), F32),
            vmem((8, 48, 256), BF16),
            vmem((8, 48, 256), BF16),
            vmem((2048, 2048), BF16),
            vmem((48, 2048), BF16),
            vmem((48, 2048), F32),
            vmem((NX, NC, 48, 2048), BF16),
            vmem((tok_rows, 704), F32),
            vmem((tok_rows, 704), F32),
            vmem((NX, NC, 48, 2048), BF16),
            vmem((NX, 48, 2048), BF16),
            vmem((6, 48, 1024), BF16),
            dma((9,)),
        ]
        + [dma((n,)) for n in sizes],
        compiler_params=pltpu.CompilerParams(
            collective_id=0, has_side_effects=True, vmem_limit_bytes=60 * 1024 * 1024
        ),
        name="whole_layer",
    )(
        kv_latent,
        kv_gain.reshape(1, -1),
        rope_key.T,
        doc_ids,
        cos_table,
        sin_table,
        q_gain.reshape(1, -1),
        mix_gain.reshape(1, -1),
        out_gain.reshape(1, -1),
        q_latent,
        w_query,
        w_key,
        w_value,
        w_gate,
        w_up,
        w_down.T,
        w_out,
        resid_stream,
    )


def solution(mesh):
    split = Mesh(mesh.devices.reshape(NZ, NY, NX, NC), ("z", "y", "x", "c"))
    in_specs = (
        P(SP, None),
        P(SP, None),
        P(SP, None),
        P(SP, None),
        P(SP),
        P(),
        P(),
        P(None, TP),
        P(None, TP),
        P(None, TP),
        P(),
        P(),
        P(SP, TP),
        P(SP, TP),
        P(TP, SP),
        P(),
    )
    out_specs = P((*SP, *TP), None)
    return jax.shard_map(body, mesh=split, in_specs=in_specs, out_specs=out_specs, check_vma=False)
```

```python
import functools
import math

import jax
import jax.numpy as jnp
from jax import lax
from jax.experimental import pallas as pl
from jax.experimental.pallas import tpu as pltpu
from jax.sharding import Mesh
from jax.sharding import PartitionSpec as P

NOPE = 128
RD = 64
VD = 128
NZ, NY, NX, NC = 8, 4, 4, 2
SP = ("z", "y")
TP = ("x", "c")
MESH = pl.DeviceIdType.MESH

eps_norm = 1e-05
rope_theta = 10000.0
resid_alpha = 8.0**0.25
HEADS_DEV = 2
WIDE = 384
A_ROWS, B_ROWS = 64, 32
EXP2_SCALE = (NOPE + RD) ** (-0.5) * math.log2(math.e)
F32 = jnp.float32
BF16 = jnp.bfloat16


def rope_angles(positions):
    lane = jnp.arange(128, dtype=jnp.int32)
    frequency = rope_theta ** (-2.0 * (lane % 32).astype(jnp.float32) / RD)
    angles = positions.astype(jnp.float32)[:, None] * frequency[None, :]
    sign = jnp.where(lane % 64 < 32, -1.0, 1.0)
    return (jnp.cos(angles), jnp.sin(angles) * sign[None, :])


def rms_scaled(latent, scaling):
    widened = latent.astype(jnp.float32)
    inverse = lax.rsqrt(jnp.mean(widened * widened, axis=-1, keepdims=True) + eps_norm)
    return (widened * inverse * scaling).astype(jnp.bfloat16)


def layer_scaled(stream, scaling):
    centre = stream - jnp.mean(stream, axis=-1, keepdims=True)
    spread = jnp.mean(centre * centre, axis=-1, keepdims=True)
    return centre * lax.rsqrt(spread + eps_norm) * scaling


class Wires:
    def __init__(self, targets):
        self.targets = targets

    def copy(self, src, dst, pair, index, way, out=0):
        send, recv = pair
        return pltpu.make_async_remote_copy(
            src_ref=src(),
            dst_ref=dst(),
            send_sem=send.at[out],
            recv_sem=recv.at[index],
            device_id=self.targets[way],
            device_id_type=MESH,
        )

    def start(self, src, dst, pair, index, way, size, out=0):
        self.copy(src, dst, pair, index, way, out).start()

    def landed(self, slot, pair, index, way):
        self.copy(slot, slot, pair, index, way).wait_recv()

    def left(self, pair, out, as_many):
        region = lambda: as_many
        self.copy(region, region, pair, 0, "c", out).wait_send()


class Ring:
    def __init__(self, wires, pair, block, me, at, part, chunk=None):
        self.w, self.pair, self.block = wires, pair, block
        self.at, self.part, self.chunk = at, part, chunk
        self.z, self.y = me
        self.yl, self.yr, self.yo = (self.y + 3) % 4, (self.y + 1) % 4, (self.y + 2) % 4
        self.zz = [(self.z + d) % 8 for d in range(8)]

    def send(self, slot, index, way, blocks):
        self.w.start(slot, slot, self.pair, index, way, blocks * self.block, int(way[0] == "z"))

    def got(self, slot, index, way="y+"):
        self.w.landed(slot, self.pair, index, way)


class RingYZ(Ring):
    def y1(self):
        own = lambda: self.at(self.z, self.y)
        self.send(own, 0, "y+", 1)
        self.send(own, 1, "y-", 1)

    def y2(self):
        self.got(lambda: self.at(self.z, self.yl), 0)
        self.got(lambda: self.at(self.z, self.yr), 1)
        self.send(lambda: self.part(self.z, self.yl, 0), 2, "y+", 0.5)
        self.send(lambda: self.part(self.z, self.yr, 1), 3, "y-", 0.5)

    def z1(self):
        self.got(lambda: self.part(self.z, self.yo, 0), 2)
        self.got(lambda: self.part(self.z, self.yo, 1), 3)
        for h in range(2):
            self.send(lambda h=h: self.half(self.z, h), 4 + 4 * h, "z+", 2)
            self.send(lambda h=h: self.half(self.z, h), 12 + 4 * h, "z-", 2)

    def half(self, a, h):
        return self.chunk(a, 2 * h, 2 * h + 2)

    def zs(self, s, h):
        right, left = self.zz[9 - s], self.zz[s - 1]
        self.got(lambda: self.half(right, h), 4 + 4 * h + s - 2)
        self.got(lambda: self.half(left, h), 12 + 4 * h + s - 2)
        if s < 4 or h == 0:
            self.send(lambda: self.half(right, h), 4 + 4 * h + s - 1, "z+", 2)
        if s < 4 or h == 1:
            self.send(lambda: self.half(left, h), 12 + 4 * h + s - 1, "z-", 2)

    def z5(self):
        self.got(lambda: self.half(self.zz[4], 0), 7)
        self.got(lambda: self.half(self.zz[4], 1), 19)

    def left(self, whole):
        self.w.left(self.pair, 0, whole.at[0, pl.ds(0, 3)])
        self.w.left(self.pair, 1, whole.at[pl.ds(0, 7)])


class RingZY(Ring):
    def z1(self):
        own = lambda: self.at(self.z, self.y)
        self.send(own, 0, "z+", 1)
        self.send(own, 4, "z-", 1)

    def zs(self, s):
        right, left = self.zz[9 - s], self.zz[s - 1]
        self.got(lambda: self.at(right, self.y), s - 2)
        self.got(lambda: self.at(left, self.y), 4 + s - 2)
        if s < 4:
            self.send(lambda: self.at(right, self.y), s - 1, "z+", 1)
            self.send(lambda: self.at(left, self.y), 4 + s - 1, "z-", 1)
        else:
            self.send(lambda: self.part(right, self.y, 0), 3, "z+", 0.5)
            self.send(lambda: self.part(left, self.y, 1), 7, "z-", 0.5)

    def z5(self):
        self.got(lambda: self.part(self.zz[4], self.y, 0), 3)
        self.got(lambda: self.part(self.zz[4], self.y, 1), 7)

    def y1(self, *steps):
        for d in steps:
            zz = self.zz[d]
            self.send(lambda zz=zz: self.at(zz, self.y), 8 + 4 * d, "y+", 1)
            self.send(lambda zz=zz: self.at(zz, self.y), 9 + 4 * d, "y-", 1)

    def y2(self, *steps):
        for d in steps:
            zz = self.zz[d]
            self.got(lambda zz=zz: self.at(zz, self.yl), 8 + 4 * d)
            self.got(lambda zz=zz: self.at(zz, self.yr), 9 + 4 * d)
            self.send(lambda zz=zz: self.part(zz, self.yl, 0), 10 + 4 * d, "y+", 0.5)
            self.send(lambda zz=zz: self.part(zz, self.yr, 1), 11 + 4 * d, "y-", 0.5)

    def y3(self, *steps):
        for d in steps:
            zz = self.zz[d]
            self.got(lambda zz=zz: self.part(zz, self.yo, 0), 10 + 4 * d)
            self.got(lambda zz=zz: self.part(zz, self.yo, 1), 11 + 4 * d)

    def left(self, whole):
        self.w.left(self.pair, 0, whole.at[pl.ds(0, 6)])
        self.w.left(self.pair, 1, whole.at[pl.ds(0, 7), 0])


def plan(ka, kb, ga, gb, across, across2, attend, stage):
    kb.z1()
    gb.z1()
    ka.y1()
    kb.y1(0)
    stage("query")
    kb.zs(2)
    kb.y1(1)
    kb.y2(0)
    ka.y2()
    kb.y1(7)
    gb.y1(0)
    gb.zs(2)
    kb.zs(3)
    kb.y1(6)
    kb.y2(1)
    kb.y3(0)
    across(1, 0)
    gb.y1(7)
    kb.y1(2)
    ka.z1()
    across(0, 0)
    kb.y3(1)
    across(1, 1)
    kb.y2(7)
    across2(1, 0)
    across2(0, 0)
    kb.y2(6)
    kb.zs(4)

    def at_0_1():
        kb.y1(3)
        ga.y1()
        ka.zs(2, 0)

    def at_1_0():
        kb.y3(7)
        across(1, 7)
        ka.zs(2, 1)
        kb.y2(2)
        across(0, 1, 7)
        kb.y1(5)
        kb.z5()
        kb.y2(3)
        kb.y3(6)
        across(1, 6)
        gb.zs(3)
        across2(1, 1)
        kb.y1(4)
        gb.y2(0)
        ka.zs(3, 0)
        ga.y2()
        kb.y2(5)
        ka.zs(3, 1)
        across(0, 2)
        kb.y3(3)
        across(1, 3)
        across2(1, 7)
        kb.y2(4)
        gb.y1(2)
        across2(0, 1)

    def at_1_1():
        gb.y1(6)
        kb.y3(2)
        across(1, 2)
        across2(0, 7)

    def at_2_0():
        across2(1, 6)
        gb.zs(4)
        across(0, 6)

    def at_2_1():
        across2(0, 2)
        kb.y3(4)
        across(1, 4)

    def at_3_0():
        across2(1, 2)
        gb.y1(1, 3)
        ka.zs(4, 0)
        across2(1, 3)
        kb.y3(5)
        across(1, 5)
        gb.y1(5)
        ka.zs(4, 1)
        across(0, 3, 5)

    def at_3_1():
        ga.z1()
        across2(0, 6)
        gb.z5()

    def at_4_1():
        across2(1, 4)
        gb.y2(7)
        across2(1, 5)
        across2(0, 3)
        ka.z5()
        across(0, 4)

    def at_5_1():
        across2(0, 5)
        gb.y2(6)

    def at_6_0():
        ga.zs(2, 0)

    def at_6_1():
        across2(0, 4)
        gb.y1(4)

    def at_7_0():
        gb.y2(2)

    def at_7_1():
        ga.zs(2, 1)

    attend(
        {
            (0, 1): at_0_1,
            (1, 0): at_1_0,
            (1, 1): at_1_1,
            (2, 0): at_2_0,
            (2, 1): at_2_1,
            (3, 0): at_3_0,
            (3, 1): at_3_1,
            (4, 1): at_4_1,
            (5, 1): at_5_1,
            (6, 0): at_6_0,
            (6, 1): at_6_1,
            (7, 0): at_7_0,
            (7, 1): at_7_1,
        }
    )
    gb.y2(1)
    stage("heads")
    gb.y2(3)
    ga.zs(3, 0)
    stage("mix")
    ga.zs(3, 1)
    stage("norm")
    gb.y2(5, 4)
    ga.zs(4, 0)
    stage("spread")
    ga.zs(4, 1)
    stage("spread2")
    gb.y3(0, 7)
    stage("gate0")
    gb.y3(6, 1)
    stage("gate1")
    ga.z5()
    gb.y3(3, 4)
    stage("gate2")
    gb.y3(5, 2)
    stage("gate3")
    stage("ffn")


def layer_kernel(
    kvl_ref,
    kvg_ref,
    rope_ref,
    doc_ref,
    cos_ref,
    sin_ref,
    qg_ref,
    mixg_ref,
    outg_ref,
    ql_ref,
    wq_ref,
    wk_ref,
    wv_ref,
    wg_ref,
    wu_ref,
    wd_ref,
    wo_ref,
    res_ref,
    out_ref,
    q_ref,
    docs,
    ropes,
    ql,
    wq,
    wk,
    wv,
    kva,
    kvb,
    wa,
    wb,
    m_ref,
    l_ref,
    acc_ref,
    att,
    heads,
    wo,
    res,
    mid,
    normed,
    gate,
    up,
    part,
    pin,
    xin,
    loc_sem,
    ka_s,
    ka_r,
    kb_s,
    kb_r,
    kp_s,
    kp_r,
    kx_s,
    kx_r,
    wa_s,
    wa_r,
    wb_s,
    wb_r,
    hd_s,
    hd_r,
    nx_s,
    nx_r,
    pp_s,
    pp_r,
    px_s,
    px_r,
):
    z, y = lax.axis_index("z"), lax.axis_index("y")
    x, c = lax.axis_index("x"), lax.axis_index("c")
    other = 1 - c
    zz = [(z + d) % 8 for d in range(8)]
    xr, xl, xo = (x + 1) % 4, (x + 3) % 4, (x + 2) % 4

    par = x % 2
    apar = 1 - par
    own_rows = pl.multiple_of(c * 192 + par * 96, 32)
    res_rows = pl.multiple_of((x * 2 + c) * 48, 48)
    local = [
        pltpu.make_async_copy(wg_ref, wa.at[z, y], loc_sem.at[2]),
        pltpu.make_async_copy(wu_ref, wb.at[z, y, 0], loc_sem.at[3]),
        pltpu.make_async_copy(wd_ref, wb.at[z, y, 1], loc_sem.at[4]),
    ]
    query_side = [
        pltpu.make_async_copy(ql_ref, ql, loc_sem.at[0]),
        pltpu.make_async_copy(wq_ref, wq, loc_sem.at[1]),
        pltpu.make_async_copy(wk_ref, wk, loc_sem.at[7]),
        pltpu.make_async_copy(wv_ref, wv, loc_sem.at[8]),
    ]
    later = [
        pltpu.make_async_copy(wo_ref, wo, loc_sem.at[5]),
        pltpu.make_async_copy(res_ref.at[pl.ds(res_rows, 48)], res, loc_sem.at[6]),
    ]
    for copy in local + query_side + later:
        copy.start()

    targets = {
        "z+": {"z": zz[1]},
        "z-": {"z": zz[7]},
        "y+": {"y": (y + 1) % 4},
        "y-": {"y": (y + 3) % 4},
        "c": {"c": other},
    }
    for dx in range(4):
        for dc in range(2):
            if dx or dc:
                targets[dx, dc] = {"x": (x + dx) % 4, "c": (c + dc) % 2}
    targets["x+"], targets["x-"] = targets[1, 0], targets[3, 0]
    barrier = pltpu.get_barrier_semaphore()
    greeted = ["z+", "z-", "y+", "y-"] + [k for k in targets if isinstance(k, tuple)]
    for way in greeted:
        pl.semaphore_signal(barrier, inc=1, device_id=targets[way], device_id_type=MESH)

    m_ref[...] = jnp.full(m_ref.shape, -1e30, F32)
    l_ref[...] = jnp.zeros(l_ref.shape, F32)
    acc_ref[...] = jnp.zeros(acc_ref.shape, F32)

    lane = lax.broadcasted_iota(jnp.int32, (384, 128), 1)
    doc_row = doc_ref[...].reshape(1, 384).astype(F32)
    docs[...] = jnp.transpose(jnp.broadcast_to(doc_row, (128, 384)))
    rope_rows = rope_ref[...].astype(F32)
    ropes[...] = jnp.transpose(jnp.concatenate([rope_rows, rope_rows], axis=0))
    own = pl.ds(own_rows, 96)
    own_lane = lane[:96]
    latent = rms_scaled(kvl_ref[own, :], kvg_ref[...])
    rope = ropes[own, :]
    turned = rope * cos_ref[own, :] + pltpu.roll(rope, 32, 1) * sin_ref[own, :]
    same = docs[own, :] == (own_lane - 64).astype(F32)
    extra = jnp.where(own_lane < 64, turned, jnp.where(same, 1.0, 0.0)).astype(BF16)
    for keys, rows in ((kva, slice(0, A_ROWS)), (kvb, slice(A_ROWS, A_ROWS + B_ROWS))):
        keys[par, c, z, y, :, 0:256] = latent[rows]
        keys[par, c, z, y, :, 256:384] = extra[rows]
    for copy in local:
        copy.wait()
    pl.semaphore_wait(barrier, len(greeted))

    wires = Wires(targets)
    me = (z, y)
    row_bytes, w_bytes = WIDE * 2, 64 * 768 * 2
    ka = RingYZ(
        wires,
        (ka_s, ka_r),
        A_ROWS * row_bytes,
        me,
        lambda a, b: kva.at[par, c, a, b],
        lambda a, b, h: kva.at[par, c, a, b, pl.ds(32 * h, 32)],
        lambda a, lo, hi: kva.at[par, c, a, pl.ds(lo, hi - lo)],
    )
    kb = RingZY(
        wires,
        (kb_s, kb_r),
        B_ROWS * row_bytes,
        me,
        lambda a, b: kvb.at[par, c, a, b],
        lambda a, b, h: kvb.at[par, c, a, b, pl.ds(16 * h, 16)],
    )
    ga = RingYZ(
        wires,
        (wa_s, wa_r),
        w_bytes,
        me,
        lambda a, b: wa.at[a, b],
        lambda a, b, h: wa.at[a, b, pl.ds(32 * h, 32)],
        lambda a, lo, hi: wa.at[a, pl.ds(lo, hi - lo)],
    )
    gb = RingZY(
        wires,
        (wb_s, wb_r),
        2 * w_bytes,
        me,
        lambda a, b: wb.at[a, b],
        lambda a, b, h: wb.at[a, b, h],
    )

    keys_of = (kva, kvb)
    core_keys, x_keys = (kp_s, kp_r), (kx_s, kx_r)

    def pair_with(color, d, theirs):
        own = apar if theirs else par
        slot = lambda: keys_of[color].at[own, c, zz[d]]
        wires.start(slot, slot, core_keys, 16 * theirs + 8 * color + d, "c", 0, 2 * theirs + color)

    def across(color, *steps):
        for d in steps:
            for h, way in ((0, "x+"), (1, "x-")):
                slot = lambda d=d, h=h: keys_of[color].at[par, c, zz[d], pl.ds(2 * h, 2)]
                wires.start(slot, slot, x_keys, 16 * h + 8 * color + d, way, 0, color)
            pair_with(color, d, 0)

    def across2(color, *steps):
        for d in steps:
            for h, way in ((0, "x+"), (1, "x-")):
                slot = lambda: keys_of[color].at[apar, c, zz[d], pl.ds(2 * h, 2)]
                wires.landed(slot, x_keys, 16 * h + 8 * color + d, way)
            pair_with(color, d, 1)

    def attend_unit(u, h):
        d = jnp.where(u % 2 == 1, (u + 1) // 2, (8 - u // 2) % 8)
        at_z = (z + d) % 8
        if h == 0:
            for theirs, own in ((0, par), (1, apar)):
                for color, keys in enumerate(keys_of):
                    wires.landed(
                        lambda: keys.at[own, other, at_z],
                        core_keys,
                        16 * theirs + 8 * color + d,
                        "c",
                    )
        rows = jnp.concatenate(
            [kva[:, :, at_z].reshape(1024, WIDE), kvb[:, :, at_z].reshape(512, WIDE)], axis=0
        )
        extra = rows[:, 256:384]
        cols_h = slice(128 * h, 128 * h + 128)
        wkv = jnp.concatenate([wk[:, cols_h], wv[:, cols_h]], axis=1)
        both = jnp.dot(rows[:, :256], wkv, preferred_element_type=F32).astype(BF16)
        keys = jnp.concatenate([both[:, :128], extra], axis=1)
        vals = both[:, 128:]
        s = lax.dot_general(
            q_ref[h], keys, (((1,), (1,)), ((), ())), preferred_element_type=F32
        )
        top_old = m_ref[h]
        top = jnp.maximum(top_old, jnp.max(s, axis=1, keepdims=True))
        factor = jnp.exp2((top_old - top) * EXP2_SCALE)
        p = jnp.exp2((s - jnp.concatenate([top] * 12, axis=1)) * EXP2_SCALE)
        total = p[:, :128]
        for k in range(1, 12):
            total = total + p[:, 128 * k : 128 * k + 128]
        m_ref[h] = top
        l_ref[h] = l_ref[h] * factor + total
        acc_ref[h] = acc_ref[h] * factor + jnp.dot(
            p.astype(BF16), vals, preferred_element_type=F32
        )

    def attend(events):
        def step(u, carry):
            for h in range(HEADS_DEV):
                for (k, at_h), event in events.items():
                    if at_h == h:
                        pl.when(u == k)(event)
                attend_unit(u, h)
            return carry

        lax.fori_loop(0, 8, step, 0)

    heads_pair, norm_pair = (hd_s, hd_r), (nx_s, nx_r)
    core_pair, x_pair = (pp_s, pp_r), (px_s, px_r)
    cols = lambda h: pl.ds(1024 * h, 1024)

    def pass_on(slot, index):
        wires.start(slot, slot, norm_pair, index, "c", 0, 1)

    def stage(name):
        if name == "query":
            for copy in query_side:
                copy.wait()
            every = jnp.dot(
                rms_scaled(ql[...], qg_ref[...]), wq[...], preferred_element_type=F32
            )
            first, mixed, last = every[:, :128], every[:, 128:256], every[:, 256:384]
            last = pltpu.roll(last, 64, 1)
            second = jnp.where(lane < 64, pltpu.roll(mixed, 64, 1), last)
            same = docs[...] == (lane - 64).astype(F32)
            apart = jnp.where(same | (lane >= 68), 0.0, -1e30)
            for h, (plain, rotary) in enumerate(((first, mixed), (second, last))):
                swapped = jnp.where(lane < 32, pltpu.roll(rotary, 96, 1), pltpu.roll(rotary, 32, 1))
                turned = rotary * cos_ref[...] + swapped * sin_ref[...]
                q_ref[h, :, 0:128] = plain.astype(BF16)
                q_ref[h, :, 128:256] = jnp.where(lane < 64, turned, apart).astype(BF16)
        if name == "heads":
            for h in range(HEADS_DEV):
                denom = jnp.sum(l_ref[h], axis=1, keepdims=True)
                done = (acc_ref[h] / denom).astype(BF16)
                att[:, :, 128 * h : 128 * h + 128] = done.reshape(8, 48, 128)
            for dx in range(4):
                for dc in range(2):
                    if dx or dc:
                        there = (x + dx) % 4 * 2 + (c + dc) % 2
                        wires.start(
                            lambda there=there: att.at[there],
                            lambda: heads.at[x * 2 + c],
                            heads_pair,
                            2 * dx + dc,
                            (dx, dc),
                            0,
                        )
            heads[x * 2 + c] = att[x * 2 + c]
        if name == "mix":
            for dx in range(4):
                for dc in range(2):
                    if dx or dc:
                        there = (x - dx + 4) % 4 * 2 + (c + dc) % 2
                        wires.landed(
                            lambda: heads.at[there], heads_pair, 2 * dx + dc, (dx, dc)
                        )
            for copy in later:
                copy.wait()
            rows = jnp.concatenate([heads[j] for j in range(8)], axis=1)

            def mix(n, carry):
                at = pl.ds(pl.multiple_of(n * 256, 256), 256)
                mid[:, at] = jnp.dot(rows, wo[:, at], preferred_element_type=F32)
                return carry

            lax.fori_loop(0, 8, mix, 0)
        if name == "norm":
            stream = resid_alpha * res[...].astype(F32) + mid[...]
            normed[x, c] = layer_scaled(stream, mixg_ref[...]).astype(BF16)
            own = lambda: normed.at[x, c]
            for index, h, way in ((0, 0, "x+"), (1, 1, "x-"), (8, 1, "x+"), (9, 0, "x-")):
                slot = lambda h=h: normed.at[x, c, :, cols(h)]
                wires.start(slot, slot, norm_pair, index, way, 0)
            pass_on(own, 4)
        if name == "spread":
            ka.left(kva.at[par, c])
            kb.left(kvb.at[par, c])
            for color, keys in enumerate(keys_of):
                wires.left(x_keys, color, keys.at[par, c])
                wires.left(core_keys, color, keys.at[par, c])
                wires.left(core_keys, 2 + color, keys.at[apar, c])
            wires.left(heads_pair, 0, heads.at[pl.ds(0, 7)])
            slot = lambda: normed.at[xl, c, :, cols(0)]
            wires.landed(slot, norm_pair, 0, "x+")
            wires.start(slot, slot, norm_pair, 2, "x+", 0)
            slot_r = lambda: normed.at[xr, c, :, cols(1)]
            wires.landed(slot_r, norm_pair, 1, "x-")
            wires.start(slot_r, slot_r, norm_pair, 3, "x-", 0)
            wires.landed(lambda: normed.at[xl, c, :, cols(1)], norm_pair, 8, "x+")
            wires.landed(lambda: normed.at[xr, c, :, cols(0)], norm_pair, 9, "x-")
            pass_on(lambda: normed.at[xl, c], 5)
            pass_on(lambda: normed.at[xr, c], 6)
        if name == "spread2":
            wires.landed(lambda: normed.at[xo, c, :, cols(0)], norm_pair, 2, "x+")
            wires.landed(lambda: normed.at[xo, c, :, cols(1)], norm_pair, 3, "x-")
            pass_on(lambda: normed.at[xo, c], 7)
            for index, at in ((4, x), (5, xl), (6, xr), (7, xo)):
                wires.landed(lambda: normed.at[at, other], norm_pair, index, "c")
        if name[:4] == "gate":
            k = int(name[4:])
            near, far = ((0, 7), (6, 1), (3, 4), (5, 2))[k]
            at = [zz[near], zz[far]]
            rows = jnp.concatenate(
                [
                    normed[:, :, :, pl.ds(pl.multiple_of(256 * a, 256), 256)].reshape(384, 256)
                    for a in at
                ],
                axis=1,
            )
            for weight, total in (
                ([wa[a].reshape(256, 704) for a in at], gate),
                ([wb[a, :, 0].reshape(256, 704) for a in at], up),
            ):
                term = jnp.dot(
                    rows, jnp.concatenate(weight, axis=0), preferred_element_type=F32
                )
                total[...] = term if k == 0 else total[...] + term
        if name == "ffn":
            v = gate[...]
            hidden = (v / (1.0 + jnp.exp(-v)) * up[...]).astype(BF16)
            for k in range(8):
                w = wb[k, :, 1].reshape(256, 704)
                term = lax.dot_general(
                    hidden, w, (((1,), (1,)), ((), ())), preferred_element_type=F32
                )
                at = pl.ds(256 * k, 256)
                part[:, :, :, at] = term.astype(BF16).reshape(4, 2, 48, 256)
                wires.start(
                    lambda at=at: part.at[:, other, :, at],
                    lambda at=at: pin.at[:, :, at],
                    core_pair,
                    k,
                    "c",
                    0,
                )
            for k in range(8):
                wires.landed(lambda: pin.at[:, :, pl.ds(256 * k, 256)], core_pair, k, "c")

            def pair_sum(at_x, lo, hi):
                return part[at_x, c, :, lo:hi].astype(F32) + pin[at_x, :, lo:hi].astype(F32)

            def x_send(index, at_x, h, way):
                wires.start(
                    lambda: pin.at[at_x, :, cols(h)], lambda: xin.at[index], x_pair, index, way, 0
                )

            for at_x, h in ((xo, 0), (xo, 1), (xr, 1), (xl, 0)):
                half = slice(1024 * h, 1024 * h + 1024)
                pin[at_x, :, half] = pair_sum(at_x, half.start, half.stop).astype(BF16)
            x_send(0, xo, 0, "x+")
            x_send(1, xo, 1, "x-")
            x_send(2, xr, 1, "x+")
            x_send(3, xl, 0, "x-")
            near_r = pair_sum(xr, 0, 1024)
            near_l = pair_sum(xl, 1024, 2048)
            wires.landed(lambda: xin.at[0], x_pair, 0, "x+")
            pin[xr, :, 0:1024] = (near_r + xin[0].astype(F32)).astype(BF16)
            x_send(4, xr, 0, "x+")
            wires.landed(lambda: xin.at[1], x_pair, 1, "x-")
            pin[xl, :, 1024:2048] = (near_l + xin[1].astype(F32)).astype(BF16)
            x_send(5, xl, 1, "x-")
            ga.left(wa)
            gb.left(wb)
            wires.left(norm_pair, 0, normed.at[pl.ds(0, 3), 0])
            wires.left(norm_pair, 1, normed.at[:, 0])
            wires.left(core_pair, 0, pin)
            for index, way in ((2, "x+"), (3, "x-"), (4, "x+"), (5, "x-")):
                wires.landed(lambda: xin.at[index], x_pair, index, way)
            low = pair_sum(x, 0, 1024) + xin[4].astype(F32) + xin[3].astype(F32)
            high = pair_sum(x, 1024, 2048) + xin[2].astype(F32) + xin[5].astype(F32)
            ffn_sum = jnp.concatenate([low, high], axis=1)
            stream = resid_alpha * normed[x, c].astype(F32) + 0.5 * ffn_sum
            out_ref[...] = layer_scaled(stream, outg_ref[...]).astype(BF16)

    plan(ka, kb, ga, gb, across, across2, attend, stage)
    wires.left(x_pair, 0, xin)


def body(
    resid_stream,
    q_latent,
    kv_latent,
    rope_key,
    doc_ids,
    q_gain,
    kv_gain,
    w_query,
    w_key,
    w_value,
    w_out,
    mix_gain,
    w_gate,
    w_up,
    w_down,
    out_gain,
):
    tok_rows = q_latent.shape[0]
    positions = lax.axis_index(SP) * tok_rows + jnp.arange(tok_rows, dtype=jnp.int32)
    cos_table, sin_table = rope_angles(positions)
    any_spec = pl.BlockSpec(memory_space=pl.ANY)
    vmem_spec = pl.BlockSpec(memory_space=pltpu.VMEM)
    dma = pltpu.SemaphoreType.DMA
    vmem = pltpu.VMEM
    sizes = (2, 20, 2, 40, 4, 32, 2, 32, 2, 20, 2, 40, 1, 8, 2, 10, 1, 8, 1, 6)
    return pl.pallas_call(
        layer_kernel,
        out_shape=jax.ShapeDtypeStruct((48, 2048), BF16),
        in_specs=[vmem_spec] * 9 + [any_spec] * 9,
        out_specs=vmem_spec,
        scratch_shapes=[
            vmem((HEADS_DEV, tok_rows, 256), BF16),
            vmem((tok_rows, 128), F32),
            vmem((tok_rows, 128), F32),
            vmem(q_latent.shape, BF16),
            vmem(w_query.shape, BF16),
            vmem(w_key.shape, BF16),
            vmem(w_value.shape, BF16),
            vmem((2, NC, NZ, NY, A_ROWS, WIDE), BF16),
            vmem((2, NC, NZ, NY, B_ROWS, WIDE), BF16),
            vmem((NZ, NY, 64, 704), BF16),
            vmem((NZ, NY, 2, 64, 704), BF16),
            vmem((HEADS_DEV, tok_rows, 128), F32),
            vmem((HEADS_DEV, tok_rows, 128), F32),
            vmem((HEADS_DEV, tok_rows, 128), F32),
            vmem((8, 48, 256), BF16),
            vmem((8, 48, 256), BF16),
            vmem((2048, 2048), BF16),
            vmem((48, 2048), BF16),
            vmem((48, 2048), F32),
            vmem((NX, NC, 48, 2048), BF16),
            vmem((tok_rows, 704), F32),
            vmem((tok_rows, 704), F32),
            vmem((NX, NC, 48, 2048), BF16),
            vmem((NX, 48, 2048), BF16),
            vmem((6, 48, 1024), BF16),
            dma((9,)),
        ]
        + [dma((n,)) for n in sizes],
        compiler_params=pltpu.CompilerParams(
            collective_id=0, has_side_effects=True, vmem_limit_bytes=60 * 1024 * 1024
        ),
        name="whole_layer",
    )(
        kv_latent,
        kv_gain.reshape(1, -1),
        rope_key.T,
        doc_ids,
        cos_table,
        sin_table,
        q_gain.reshape(1, -1),
        mix_gain.reshape(1, -1),
        out_gain.reshape(1, -1),
        q_latent,
        w_query,
        w_key,
        w_value,
        w_gate,
        w_up,
        w_down.T,
        w_out,
        resid_stream,
    )


def solution(mesh):
    split = Mesh(mesh.devices.reshape(NZ, NY, NX, NC), ("z", "y", "x", "c"))
    in_specs = (
        P(SP, None),
        P(SP, None),
        P(SP, None),
        P(SP, None),
        P(SP),
        P(),
        P(),
        P(None, TP),
        P(None, TP),
        P(None, TP),
        P(),
        P(),
        P(SP, TP),
        P(SP, TP),
        P(TP, SP),
        P(),
    )
    out_specs = P((*SP, *TP), None)
    return jax.shard_map(body, mesh=split, in_specs=in_specs, out_specs=out_specs, check_vma=False)
```
